32 devices in a mesh: fs: 8 (over z, y), tp: 4 (over x, core).
Axes of the slice: x: 2, y: 2, z: 4, core: 2. Of those that a mesh axis runs over, the one named last changes fastest.
Arguments:
- tokens: bfloat16 [6144, 2048], P('fs'), may hold values from -6 to 6
- routes: int32 [6144, 2], P('fs'), may hold values from 0 to 7, all different within a row; in each aligned block of 768 rows (0 to 767, 768 to 1535, ...) at most 216 rows name the same one
- route_weight: float32 [6144, 2], P('fs'), may hold values from 0.2 to 1
- norm_gain: float32 [2048], P('fs'), may hold values from 0.1 to 1.9
- gate_master: float32 [8, 2048, 4096], P(None, 'fs', 'tp'), may hold values from -0.125 to 0.125
- up_master: float32 [8, 2048, 4096], P(None, 'fs', 'tp'), may hold values from -0.125 to 0.125
- down_master: float32 [8, 4096, 2048], P(None, 'fs', 'tp'), may hold values from -0.09375 to 0.09375
Outputs:
- gate_serve: bfloat16 [8, 2048, 4096], P('fs', None, 'tp')
- up_serve: bfloat16 [8, 2048, 4096], P('fs', None, 'tp')
- down_serve: bfloat16 [8, 4096, 2048], P('fs', 'tp')
- layer_out: bfloat16 [6144, 2048], P('fs', 'tp')
The draws below stay inside these ranges and needn't reach their ends.
Inputs may be any that keep to these rules, and one draw needn't show every extreme that they name: `routes`: each row names two different experts; among the 768 rows of one index of fs no expert is named by more than 216 rows, a bound that some block reaches.
All inputs are finite; a program needn't handle non-finite values.
Results may differ from the reference program's by a relative error of at most 0.015.
Values may be sent and summed in bfloat16 or wider, within the bound.
A program may use at most 192 MiB of HBM per device.

```python
import math
import jax
import jax.numpy as jnp
import numpy as np
from jax import lax

D = 2048
FF = 4096
TOK_DEV = 768
CAP = 216
EXPERTS = 8
TOKENS = 6144
N_FS = 8
N_TP = 4


def block_scale(key, extent, shards, low, largest):
    loudness, own = 1.0, jax.random.fold_in(key, 6)
    for axis_at, parts in shards:
        draws = jnp.exp(jax.random.uniform(jax.random.fold_in(own, axis_at), (parts,), jnp.float32, low / len(shards), largest / len(shards)))
        loudness = loudness * jnp.repeat(draws, extent[axis_at] // parts).reshape([-1 if axis == axis_at else 1 for axis in range(len(extent))])
    return loudness


def deal_out(key, own, number, rows, count, top, reach, slope):
    order = jax.random.permutation(key, count)
    crowded, usual = portions_of(count, rows * top, reach, slope, True), portions_of(count, rows * top, reach, slope, False)
    places = jnp.arange(count)

    def named(lengths, turn):
        used = int((lengths > 0).sum())
        fixed = max(1, used // 4)
        passed = fixed + (places - fixed + turn * (used - fixed)) % max(1, count - fixed)
        return jnp.zeros((count,), jnp.int32).at[order[jnp.where(places < fixed, places, passed)]].set(jnp.asarray(lengths, jnp.int32))

    lengths = jnp.where(number % 4 == 0, named(crowded, number // 4), named(usual, number - number // 4 - 1))
    mixed = jax.random.permutation(jax.random.fold_in(own, 3), count)
    donor, sink = mixed[0:count // 2 * 2:2], mixed[1:count // 2 * 2:2]
    margin = jnp.minimum(lengths[donor] - 1, reach - lengths[sink]) // 2
    margin = jnp.where((donor == order[0]) | (sink == order[0]) | (lengths[sink] == 0), 0, jnp.maximum(margin, 0))
    passed = jax.random.randint(jax.random.fold_in(own, 4), (count // 2,), 0, 1 << 20) % (margin + 1)
    lengths = lengths.at[donor].add(-passed).at[sink].add(passed)
    labels = jnp.searchsorted(jnp.cumsum(lengths), jnp.arange(rows * top), side="right").astype(jnp.int32)
    table = labels.reshape(top, rows).T
    table = table[jax.random.permutation(jax.random.fold_in(own, 1), rows)]
    turn = jax.random.randint(jax.random.fold_in(own, 2), (rows, 1), 0, top)
    return jnp.take_along_axis(table, (jnp.arange(top)[None, :] + turn) % top, axis=1)


def portions_of(count, total, reach, slope, full):
    weights = [(1 << 20) // math.isqrt(rank ** slope) + 1 for rank in range(1, count + 1)]
    largest = reach if full else min(reach, max(-(-total // count), total * weights[0] // sum(weights)))
    least = 1 if total - largest >= count - 1 else 0
    holding, rest = [largest] + [least] * (count - 1), total - largest - least * (count - 1)
    while rest > 0:
        movable = [i for i in range(1, count) if holding[i] < largest] or [i for i in range(1, count) if holding[i] < reach]
        pool, remaining = sum([weights[i] for i in movable]), rest
        for i in movable:
            extra = min(reach - holding[i], max(1, remaining * weights[i] // pool), rest)
            holding[i] = holding[i] + extra
            rest = rest - extra
    return np.array(holding)


def centred(own_key, dims, deviation, most, pieces=(), kind=jnp.bfloat16):
    result = deviation * jax.random.normal(own_key, dims, jnp.float32)
    if pieces:
        result = result * block_scale(own_key, dims, pieces, -0.22, 0.18)
    return jnp.clip(result, -most, most).astype(kind)


def setup_inputs(seed: int = 0) -> dict:
    key_of = jax.random.split(jax.random.key(seed), 8)
    tokens = centred(key_of[0], (TOKENS, D), 1.0, 6.0, ((0, 8),))
    routes_keys = jax.random.split(jax.random.fold_in(key_of[1], 1), TOKENS // TOK_DEV)
    routes_turns = jax.random.permutation(jax.random.fold_in(key_of[1], 3), TOKENS // TOK_DEV)
    routes = jax.vmap(lambda own, number: deal_out(jax.random.fold_in(key_of[1], 2), own, number, TOK_DEV, EXPERTS, 2, CAP, 2))(routes_keys, routes_turns).reshape((TOKENS, 2))
    route_weight = jnp.clip(0.2 + 0.8 * jax.random.uniform(key_of[2], (TOKENS, 2), jnp.float32) ** block_scale(key_of[2], (TOKENS, 2), ((0, 8),), -0.2, 0.2), 0.2, 1.0)
    norm_gain = jnp.clip(1.0 + 0.18 * jax.random.normal(key_of[3], (D,), jnp.float32), 0.1, 1.9)
    gate_master = centred(key_of[4], (EXPERTS, D, FF), D ** -0.5, 0.125, ((1, 8), (2, 4)), jnp.float32)
    up_master = centred(key_of[5], (EXPERTS, D, FF), D ** -0.5, 0.125, ((1, 8), (2, 4)), jnp.float32)
    down_master = centred(key_of[6], (EXPERTS, FF, D), FF ** -0.5, 0.09375, ((1, 8), (2, 4)), jnp.float32)
    return dict(tokens=tokens, routes=routes, route_weight=route_weight, norm_gain=norm_gain, gate_master=gate_master, up_master=up_master, down_master=down_master)


def reference(tokens, routes, route_weight, norm_gain, gate_master, up_master, down_master):
    values = tokens.astype(jnp.float32)
    normed = (values * lax.rsqrt(lax.optimization_barrier(jnp.mean(values * values, axis=-1, keepdims=True)) + 1e-06)).astype(jnp.bfloat16)
    gate_serve = (norm_gain[None, :, None] * gate_master).astype(jnp.bfloat16)
    up_serve = (norm_gain[None, :, None] * up_master).astype(jnp.bfloat16)
    down_serve = down_master.astype(jnp.bfloat16)
    rows_cap = N_FS * CAP
    group_units = FF // N_TP

    def expert_step(totals, expert):
        is_routed = jnp.any(routes == expert, axis=1)
        ordering = jnp.argsort(jnp.where(is_routed, 0, 1).astype(jnp.int32), stable=True)[:rows_cap]
        present = is_routed[ordering]
        chosen_rows = jnp.where(present[:, None], normed[ordering], jnp.zeros((), jnp.bfloat16))
        gate_pre = jnp.dot(chosen_rows, gate_serve[expert], preferred_element_type=jnp.float32)
        up_pre = jnp.dot(chosen_rows, up_serve[expert], preferred_element_type=jnp.float32)
        hidden = (jax.nn.silu(gate_pre) * up_pre).astype(jnp.bfloat16)
        block_sums = jnp.einsum('rgf,gfd->grd', hidden.reshape(rows_cap, N_TP, group_units).astype(jnp.float32), down_serve[expert].reshape(N_TP, group_units, D).astype(jnp.float32))
        rounded = lax.optimization_barrier(block_sums.astype(jnp.bfloat16)).astype(jnp.float32)
        expert_out = lax.optimization_barrier(jnp.sum(rounded, axis=0)).astype(jnp.bfloat16)
        row_weight = lax.optimization_barrier(jnp.sum(jnp.where(routes[ordering] == expert, route_weight[ordering], jnp.zeros((), jnp.float32)), axis=1))
        row_weight = jnp.where(present, row_weight, jnp.zeros((), jnp.float32))
        totals = totals.at[ordering].add(row_weight[:, None] * expert_out.astype(jnp.float32))
        return (totals, None)
    totals, _ = lax.scan(expert_step, jnp.zeros((TOKENS, D), jnp.float32), jnp.arange(EXPERTS, dtype=jnp.int32))
    return (gate_serve, up_serve, down_serve, totals.astype(jnp.bfloat16))
```

```python
import functools

import jax
import jax.numpy as jnp
from jax import lax
from jax.experimental import pallas as pl
from jax.experimental.pallas import tpu as pltpu
from jax.sharding import PartitionSpec as P

CAP = 216
ROWS = 224
DEPTH = 256
LANES = 128
STAGES = 3
MESH = pl.DeviceIdType.MESH
F32, BF16 = jnp.float32, jnp.bfloat16


def aligned(value, step=LANES):
    return pl.multiple_of(value, step)


def kernel(
    n_fs, n_tp, routes_in, routes_across_in, weight_in, gain_in, tokens_in, gate_in, up_in, down_in,
    gate_out, up_out, down_out, layer_out,
    gate_send, gate_recv, up_send, up_recv, down_send, down_recv, stage, down_stage,
    tokens, normed, outgoing, incoming, hidden, far, far_recv, near, across_recv,
    back_send, back_recv, result, gain_row, gain, routes, routes_across, weight, slot_across, slot, share,
    load_sem, down_load_sem, small_sem, gate_ss, gate_rs, up_ss, up_rs, token_ss, token_rs,
    down_ss, down_rs, line_ss, line_rs, pair_ss, pair_rs, far_ss, far_rs, across_ss, across_rs,
    back_ss, back_rs, gate_os, up_os, down_os, out_sem,
):
    f, t = lax.axis_index("fs"), lax.axis_index("tp")
    core, x = t % 2, t // 2
    chips = n_tp // 2
    ratio = n_fs // n_tp
    rows, units = gate_send.shape[1:]
    part = down_stage.shape[1]
    columns = down_stage.shape[2]
    chunks = columns // LANES
    count = tokens.shape[0]
    half = n_fs // 2

    def remote(src, dst, ss, rs, fs, tp):
        return pltpu.make_async_remote_copy(
            src_ref=src, dst_ref=dst, send_sem=ss, recv_sem=rs,
            device_id={"fs": fs, "tp": tp}, device_id_type=MESH,
        )

    def each(n, action):
        def step(i, carry):
            action(i)
            return carry

        lax.fori_loop(0, n, step, 0)

    def offset(i):
        return jnp.where(i < half, i + half, jnp.where(i == n_fs - 1, 0, i - half + 1))

    small = [
        pltpu.make_async_copy(gain_in, gain_row, small_sem.at[0]),
        pltpu.make_async_copy(routes_in, routes, small_sem.at[1]),
        pltpu.make_async_copy(routes_across_in, routes_across, small_sem.at[2]),
        pltpu.make_async_copy(weight_in, weight, small_sem.at[3]),
        pltpu.make_async_copy(tokens_in, tokens, small_sem.at[4]),
    ]
    small[0].start()

    def load(source, i):
        return pltpu.make_async_copy(
            source.at[jnp.bitwise_xor(f, offset(i))], stage.at[i % STAGES], load_sem.at[i % STAGES]
        )

    for i in range(STAGES):
        load(gate_in, i).start()
    for copy in small[1:]:
        copy.start()

    barrier = pltpu.get_barrier_semaphore()
    total = n_fs * n_tp
    me = f * n_tp + t

    def greet(i):
        other = (me + i + 1) % total
        pl.semaphore_signal(
            barrier, inc=1, device_id={"fs": other // n_tp, "tp": other % n_tp}, device_id_type=MESH
        )

    each(total - 1, greet)

    back_recv[:, :, CAP:, :] = jnp.zeros((chunks, n_fs, DEPTH - CAP, LANES), BF16)

    small[0].wait()
    same = lax.broadcasted_iota(jnp.int32, (rows, rows), 0) == lax.broadcasted_iota(jnp.int32, (rows, rows), 1)
    column = jnp.sum(jnp.where(same, gain_row[...], 0.0), axis=1, keepdims=True)
    gain[...] = jnp.broadcast_to(column, (rows, LANES))

    def weight_copy(send, recv, ss, rs, e, owner):
        return remote(
            send.at[e], recv.at[pl.ds(aligned(owner * rows), rows)], ss.at[e], rs.at[owner], e, t
        )

    def scaled(block):
        scale = gain[...]
        return jnp.concatenate(
            [(block[:, k : k + LANES] * scale).astype(BF16) for k in range(0, units, LANES)], axis=1
        )

    def send_weights(source, following, send, recv, ss, rs):
        def step(i):
            e = jnp.bitwise_xor(f, offset(i))
            load(source, i).wait()
            cast = scaled(stage[i % STAGES])

            @pl.when(i < n_fs - 1)
            def _():
                send[e] = cast

            @pl.when(i == n_fs - 1)
            def _():
                recv[pl.ds(aligned(f * rows), rows), :] = cast

            @pl.when(i + STAGES < n_fs)
            def _():
                load(source, i + STAGES).start()

            if following is not None:

                @pl.when(i + STAGES >= n_fs)
                def _():
                    j = i + STAGES - n_fs
                    pltpu.make_async_copy(
                        following.at[jnp.bitwise_xor(f, offset(j))],
                        stage.at[i % STAGES],
                        load_sem.at[i % STAGES],
                    ).start()

            if ss is not None:

                @pl.when(i > 0)
                def _():
                    weight_copy(send, recv, ss, rs, jnp.bitwise_xor(f, offset(i - 1)), f).start()

        return step

    pl.semaphore_wait(barrier, total - 1)
    each(n_fs, send_weights(gate_in, None, gate_send, gate_recv, gate_ss, gate_rs))
    for i in range(STAGES):
        load(up_in, i).start()

    for copy in small[1:4]:
        copy.wait()
    row_id = lax.broadcasted_iota(jnp.int32, (count, count), 0)
    column_id = lax.broadcasted_iota(jnp.int32, (count, count), 1)
    expert_row = lax.broadcasted_iota(jnp.int32, (n_fs, count), 0)
    named = (expert_row == routes_across[0:1, :]) | (expert_row == routes_across[1:2, :])
    before = jnp.dot(
        jnp.where(named, 1.0, 0.0).astype(BF16),
        jnp.where(row_id < column_id, 1.0, 0.0).astype(BF16),
        preferred_element_type=F32,
    )
    slot_across[...] = jnp.where(named, before, -1.0)
    expert_lane = lax.broadcasted_iota(jnp.int32, (count, LANES), 1)
    first, second = expert_lane == routes[:, 0:1], expert_lane == routes[:, 1:2]
    before = jnp.dot(
        jnp.where(column_id < row_id, 1.0, 0.0).astype(BF16),
        jnp.where(first | second, 1.0, 0.0).astype(BF16),
        preferred_element_type=F32,
    )
    slot[...] = jnp.where(first | second, before, -1.0)
    share[...] = jnp.where(first, weight[:, 0:1], 0.0) + jnp.where(second, weight[:, 1:2], 0.0)

    small[4].wait()
    strip = 96

    def norm(i):
        at = pl.ds(aligned(i * strip, strip), strip)
        values = tokens[at, :].astype(F32)
        scale = lax.rsqrt(jnp.mean(values * values, axis=1, keepdims=True) + 1e-06)
        mine = tokens[at, pl.ds(aligned(t * columns), columns)].astype(F32)
        normed[at, :] = (mine * scale).astype(BF16)

    each(count // strip, norm)

    def token_copy(e, owner):
        return remote(
            outgoing.at[e, pl.ds(0, CAP)],
            incoming.at[owner, pl.ds(0, CAP), pl.ds(aligned(t * columns), columns)],
            token_ss.at[e],
            token_rs.at[owner],
            e,
            t,
        )

    slot_id = lax.broadcasted_iota(jnp.int32, (ROWS, count), 0).astype(F32)

    def dispatch(i):
        e = jnp.bitwise_xor(f, offset(i))
        pick = jnp.where(slot_id == slot_across[pl.ds(e, 1), :], 1.0, 0.0).astype(BF16)
        picked = jnp.dot(pick, normed[...], preferred_element_type=F32).astype(BF16)

        @pl.when(i < n_fs - 1)
        def _():
            outgoing[e] = picked

        @pl.when(i == n_fs - 1)
        def _():
            incoming[f, :, pl.ds(aligned(t * columns), columns)] = picked

        @pl.when(i > 0)
        def _():
            token_copy(jnp.bitwise_xor(f, offset(i - 1)), f).start()

    each(n_fs, dispatch)

    each(n_fs, send_weights(up_in, None, up_send, up_recv, up_ss, up_rs))

    def down_load(i):
        return pltpu.make_async_copy(down_in.at[i], down_stage.at[i % 2], down_load_sem.at[i % 2])

    owner = f // ratio

    def place(tp):
        return aligned((tp % 2 * chips + tp // 2) * LANES)

    def down_copy(c, e, to, fs, tp):
        return remote(
            down_send.at[c, e],
            down_recv.at[c, pl.ds(aligned(fs % ratio * part), part), pl.ds(place(tp), LANES)],
            down_ss.at[c, e],
            down_rs.at[c, fs % ratio * n_tp + tp],
            e,
            to,
        )

    down_load(0).start()
    down_load(1).start()

    def down_cast(i):
        down_load(i).wait()
        for c in range(chunks):
            down_send[c, i] = down_stage[i % 2, :, c * LANES : (c + 1) * LANES].astype(BF16)

        @pl.when(i + 2 < n_fs)
        def _():
            down_load(i + 2).start()

    each(n_fs, down_cast)

    def send_down(c):
        def one(i):
            e = jnp.bitwise_xor(f, offset(i))
            mine = (e == f) & (owner == t)

            @pl.when(mine)
            def _():
                down_recv[c, pl.ds(aligned(f % ratio * part), part), pl.ds(place(t), LANES)] = down_send[c, e]

            @pl.when(jnp.logical_not(mine))
            def _():
                down_copy(c, e, owner, f, t).start()

        each(n_fs, one)

    def peers(action):
        each(n_fs - 1, lambda i: action(jnp.bitwise_xor(f, i + 1)))

    peers(lambda e: token_copy(e, e).wait_recv())

    def span(tp):
        return incoming.at[:, pl.ds(0, CAP), pl.ds(aligned(tp * columns), columns)]

    def line(d, chip):
        other = jnp.bitwise_xor(x, d)
        return remote(
            span(chip * 2 + core), span(chip * 2 + core), line_ss.at[d - 1], line_rs.at[d - 1], f, other * 2 + core
        )

    def pair(d, on):
        chip = jnp.bitwise_xor(x, d)
        return remote(
            span(chip * 2 + on), span(chip * 2 + on), pair_ss.at[d], pair_rs.at[d], f, x * 2 + 1 - core
        )

    for d in range(1, chips):
        line(d, x).start()
    pair(0, core).start()
    send_down(0)
    for d in range(1, chips):
        line(d, jnp.bitwise_xor(x, d)).wait_recv()
        pair(d, core).start()
    for d in range(chips):
        pair(d, 1 - core).wait_recv()

    peers(lambda e: weight_copy(gate_send, gate_recv, gate_ss, gate_rs, e, e).wait_recv())
    gate_store = pltpu.make_async_copy(gate_recv, gate_out, gate_os)
    gate_store.start()
    peers(lambda e: weight_copy(up_send, up_recv, up_ss, up_rs, e, e).wait_recv())
    up_store = pltpu.make_async_copy(up_recv, up_out, up_os)
    up_store.start()
    for c in range(1, chunks):
        send_down(c)

    tile = 256
    width = incoming.shape[2]
    group = 2

    def hidden_step(i):
        g, n = i // (units // tile), i % (units // tile)
        lanes = pl.ds(aligned(n * tile, tile), tile)
        at = pl.ds(g * group, group)
        received = incoming[at].reshape(group * ROWS, width)
        gate_pre = jnp.dot(received, gate_recv[:, lanes], preferred_element_type=F32)
        up_pre = jnp.dot(received, up_recv[:, lanes], preferred_element_type=F32)
        value = gate_pre / (1.0 + jnp.exp(-gate_pre)) * up_pre
        hidden[at, :, lanes] = value.astype(BF16).reshape(group, ROWS, tile)

    each(n_fs // group * (units // tile), hidden_step)

    def far_copy(c):
        return remote(far, far_recv.at[c], far_ss.at[c], far_rs.at[c], f, x * 2 + 1 - core)

    def across_copy(c, d):
        other = jnp.bitwise_xor(x, d)
        return remote(
            near.at[other], across_recv.at[c, d - 1], across_ss.at[c, d - 1], across_rs.at[c, d - 1],
            f, other * 2 + core,
        )

    def back_copy(c, e, owner):
        return remote(
            back_send.at[c, e, pl.ds(0, CAP)],
            back_recv.at[c, owner, pl.ds(0, CAP)],
            back_ss.at[c, e],
            back_rs.at[c, owner],
            e,
            t,
        )

    def send_back(c):
        peers(lambda e: back_copy(c, e, f).start())

    def down_store(c, tp):
        return pltpu.make_async_copy(
            down_recv.at[c, :, pl.ds(place(tp), LANES)],
            down_out.at[:, pl.ds(aligned(tp * columns + c * LANES), LANES)],
            down_os.at[c, tp],
        )

    def product(c, side, target):
        lanes = pl.ds(aligned(side * (chips * LANES)), chips * LANES)

        def step(g):
            at = pl.ds(g * group, group)
            value = jnp.dot(
                hidden[at].reshape(group * ROWS, units), down_recv[c, :, lanes], preferred_element_type=F32
            ).astype(BF16)
            for chip in range(chips):
                target[chip, at] = value[:, chip * LANES : (chip + 1) * LANES].reshape(group, ROWS, LANES)

        each(n_fs // group, step)

    def down_chunk(c):
        def arrival(i):
            fs, tp = owner_first + i // n_tp, i % n_tp

            @pl.when(jnp.logical_not((fs == f) & (tp == t)))
            def _():
                down_copy(c, f, t, fs, tp).wait_recv()

        owner_first = t * ratio
        each(ratio * n_tp, arrival)
        each(n_tp, lambda tp: down_store(c, tp).start())

        @pl.when(c == chunks - 1)
        def _():
            each(chunks - 1, send_back)

        product(c, 1 - core, far)
        far_copy(c).start()

        @pl.when(c > 0)
        def _():
            for d in range(1, chips):
                across_copy(c - 1, d).wait_send()

        product(c, core, near)
        far_copy(c).wait()
        for d in range(1, chips):
            other = jnp.bitwise_xor(x, d)

            def add(e):
                near[other, e] = (near[other, e].astype(F32) + far_recv[c, other, e].astype(F32)).astype(BF16)

            each(n_fs, add)
            across_copy(c, d).start()
        for d in range(1, chips):
            across_copy(c, d).wait_recv()

        def finish(e):
            value = near[x, e].astype(F32) + far_recv[c, x, e].astype(F32)
            for d in range(1, chips):
                value = value + across_recv[c, d - 1, e].astype(F32)
            back_send[c, e] = value.astype(BF16)

        each(n_fs, finish)
        back_recv[c, f, pl.ds(0, CAP), :] = back_send[c, f, pl.ds(0, CAP), :]

    each(chunks, down_chunk)
    send_back(chunks - 1)
    for d in range(1, chips):
        across_copy(chunks - 1, d).wait_send()

    lane_id = lax.broadcasted_iota(jnp.int32, (count, DEPTH), 1).astype(F32)

    def out_copy(c):
        return pltpu.make_async_copy(
            result.at[c], layer_out.at[:, pl.ds(aligned(c * LANES), LANES)], out_sem.at[c]
        )

    def combine(c):
        peers(lambda e: back_copy(c, e, e).wait_recv())
        value = jnp.zeros((count, LANES), F32)
        for e in range(n_fs):
            pick = jnp.where(lane_id == slot[:, e : e + 1], 1.0, 0.0).astype(BF16)
            value = value + share[:, e : e + 1] * jnp.dot(pick, back_recv[c, e], preferred_element_type=F32)
        result[c] = value.astype(BF16)
        out_copy(c).start()

    each(chunks, combine)

    peers(lambda e: weight_copy(gate_send, gate_recv, gate_ss, gate_rs, e, f).wait_send())
    peers(lambda e: weight_copy(up_send, up_recv, up_ss, up_rs, e, f).wait_send())
    peers(lambda e: token_copy(e, f).wait_send())
    for d in range(1, chips):
        line(d, x).wait_send()
    for d in range(chips):
        pair(d, core).wait_send()

    def drain(c):
        def one(e):
            @pl.when(jnp.logical_not((e == f) & (owner == t)))
            def _():
                down_copy(c, e, owner, f, t).wait_send()

        each(n_fs, one)
        each(n_tp, lambda tp: down_store(c, tp).wait())
        peers(lambda e: back_copy(c, e, f).wait_send())
        out_copy(c).wait()

    each(chunks, drain)
    gate_store.wait()
    up_store.wait()


def body(tokens, routes, route_weight, norm_gain, gate_master, up_master, down_master):
    n_fs, n_tp = lax.axis_size("fs"), lax.axis_size("tp")
    count, width = tokens.shape
    experts, rows, units = gate_master.shape
    part, columns = down_master.shape[1:]
    chips, chunks, ratio = n_tp // 2, columns // LANES, n_fs // n_tp
    assert experts == n_fs
    dma = pltpu.SemaphoreType.DMA
    lines = max(1, chips - 1)
    scratch = [
        pltpu.VMEM((n_fs, rows, units), BF16),
        pltpu.VMEM((n_fs * rows, units), BF16),
        pltpu.VMEM((n_fs, rows, units), BF16),
        pltpu.VMEM((n_fs * rows, units), BF16),
        pltpu.VMEM((chunks, n_fs, part, LANES), BF16),
        pltpu.VMEM((chunks, ratio * part, n_tp * LANES), BF16),
        pltpu.VMEM((STAGES, rows, units), F32),
        pltpu.VMEM((2, part, columns), F32),
        pltpu.VMEM((count, width), BF16),
        pltpu.VMEM((count, columns), BF16),
        pltpu.VMEM((n_fs, ROWS, columns), BF16),
        pltpu.VMEM((n_fs, ROWS, width), BF16),
        pltpu.VMEM((n_fs, ROWS, units), BF16),
        pltpu.VMEM((chips, n_fs, ROWS, LANES), BF16),
        pltpu.VMEM((chunks, chips, n_fs, ROWS, LANES), BF16),
        pltpu.VMEM((chips, n_fs, ROWS, LANES), BF16),
        pltpu.VMEM((chunks, lines, n_fs, ROWS, LANES), BF16),
        pltpu.VMEM((chunks, n_fs, ROWS, LANES), BF16),
        pltpu.VMEM((chunks, n_fs, DEPTH, LANES), BF16),
        pltpu.VMEM((chunks, count, LANES), BF16),
        pltpu.VMEM((1, rows), F32),
        pltpu.VMEM((rows, LANES), F32),
        pltpu.VMEM((count, 2), jnp.int32),
        pltpu.VMEM((2, count), jnp.int32),
        pltpu.VMEM((count, 2), F32),
        pltpu.VMEM((n_fs, count), F32),
        pltpu.VMEM((count, LANES), F32),
        pltpu.VMEM((count, LANES), F32),
        dma((STAGES,)), dma((2,)), dma((5,)),
        dma((n_fs,)), dma((n_fs,)), dma((n_fs,)), dma((n_fs,)), dma((n_fs,)), dma((n_fs,)),
        dma((chunks, n_fs)), dma((chunks, ratio * n_tp)),
        dma((lines,)), dma((lines,)), dma((chips,)), dma((chips,)),
        dma((chunks,)), dma((chunks,)), dma((chunks, lines)), dma((chunks, lines)),
        dma((chunks, n_fs)), dma((chunks, n_fs)),
        dma, dma, dma((chunks, n_tp)), dma((chunks,)),
    ]
    anywhere = pl.BlockSpec(memory_space=pl.ANY)
    return pl.pallas_call(
        functools.partial(kernel, n_fs, n_tp),
        out_shape=(
            jax.ShapeDtypeStruct((n_fs * rows, units), BF16),
            jax.ShapeDtypeStruct((n_fs * rows, units), BF16),
            jax.ShapeDtypeStruct((ratio * part, n_tp * columns), BF16),
            jax.ShapeDtypeStruct((count, columns), BF16),
        ),
        in_specs=[anywhere] * 8,
        out_specs=(anywhere,) * 4,
        scratch_shapes=scratch,
        compiler_params=pltpu.CompilerParams(
            collective_id=0, has_side_effects=True, vmem_limit_bytes=67043328
        ),
        name="layer",
    )(routes, routes.T, route_weight, norm_gain[None], tokens, gate_master, up_master, down_master)


def solution(mesh):
    placed = (
        P("fs", None),
        P("fs", None),
        P("fs", None),
        P("fs"),
        P(None, "fs", "tp"),
        P(None, "fs", "tp"),
        P(None, "fs", "tp"),
    )

    def step(*args):
        gate, up, down, out = body(*args)
        return gate[None], up[None], down[None], out

    return jax.shard_map(
        step,
        mesh=mesh,
        in_specs=placed,
        out_specs=(P("fs", None, "tp"), P("fs", None, "tp"), P("fs", "tp", None), P("fs", "tp")),
        check_vma=False,
    )
```

```python
import functools

import jax
import jax.numpy as jnp
from jax import lax
from jax.experimental import pallas as pl
from jax.experimental.pallas import tpu as pltpu
from jax.sharding import PartitionSpec as P

CAP = 216
ROWS = 224
DEPTH = 256
LANES = 128
STAGES = 3
VMEM = 67 * 1000 * 1000
MESH = pl.DeviceIdType.MESH
F32, BF16 = jnp.float32, jnp.bfloat16


def aligned(value, step=LANES):
    return pl.multiple_of(value, step)


def kernel(
    n_fs, n_tp, routes_in, weight_in, gain_in, tokens_in, gate_in, up_in, down_in,
    gate_recv, up_recv, down_recv, result,
    gate_send, up_send, down_send, stage, down_stage,
    tokens, normed, outgoing, incoming, hidden, far, far_recv, near, across_recv,
    back_send, back_recv, gain_row, gain, routes, weight, slot_across, slot, share,
    load_sem, down_load_sem, small_sem, token_load_sem, gate_ss, gate_rs, up_ss, up_rs, token_ss, token_rs,
    down_ss, down_rs, line_ss, line_rs, pair_ss, pair_rs, far_ss, far_rs, across_ss, across_rs,
    back_ss, back_rs,
):
    f, t = lax.axis_index("fs"), lax.axis_index("tp")
    core, x = t % 2, t // 2
    chips = n_tp // 2
    ratio = n_fs // n_tp
    rows, units = gate_send.shape[1:]
    part = down_stage.shape[1]
    columns = down_stage.shape[2]
    chunks = columns // LANES
    half = n_fs // 2

    def remote(src, dst, ss, rs, fs, tp):
        return pltpu.make_async_remote_copy(
            src_ref=src, dst_ref=dst, send_sem=ss, recv_sem=rs,
            device_id={"fs": fs, "tp": tp}, device_id_type=MESH,
        )

    def each(n, action):
        def step(i, carry):
            action(i)
            return carry

        lax.fori_loop(0, n, step, 0)

    def offset(i):
        return jnp.where(i < half, i + half, jnp.where(i == n_fs - 1, 0, i - half + 1))

    small = [
        pltpu.make_async_copy(gain_in, gain_row, small_sem.at[0]),
        pltpu.make_async_copy(routes_in, routes, small_sem.at[1]),
        pltpu.make_async_copy(weight_in, weight, small_sem.at[2]),
    ]
    small[0].start()

    def load(source, i):
        return pltpu.make_async_copy(
            source.at[jnp.bitwise_xor(f, offset(i))], stage.at[i % STAGES], load_sem.at[i % STAGES]
        )

    for i in range(STAGES):
        load(gate_in, i).start()
    for copy in small[1:]:
        copy.start()
    strip = tokens.shape[1]
    count = normed.shape[0]

    def token_load(i):
        return pltpu.make_async_copy(
            tokens_in.at[pl.ds(aligned(i * strip, strip), strip)], tokens.at[i % 2], token_load_sem.at[i % 2]
        )

    token_load(0).start()
    token_load(1).start()

    barrier = pltpu.get_barrier_semaphore()
    total = n_fs * n_tp
    me = f * n_tp + t

    def greet(i):
        other = (me + i + 1) % total
        pl.semaphore_signal(
            barrier, inc=1, device_id={"fs": other // n_tp, "tp": other % n_tp}, device_id_type=MESH
        )

    each(total - 1, greet)

    back_recv[:, :, CAP:, :] = jnp.zeros((chunks, n_fs, DEPTH - CAP, LANES), BF16)

    small[0].wait()
    same = lax.broadcasted_iota(jnp.int32, (rows, rows), 0) == lax.broadcasted_iota(jnp.int32, (rows, rows), 1)
    column = jnp.sum(jnp.where(same, gain_row[...], 0.0), axis=1, keepdims=True)
    gain[...] = jnp.broadcast_to(column, (rows, LANES))

    def weight_copy(send, recv, ss, rs, e, owner):
        return remote(
            send.at[e], recv.at[pl.ds(aligned(owner * rows), rows)], ss.at[e], rs.at[owner], e, t
        )

    def scaled(block):
        scale = gain[...]
        return jnp.concatenate(
            [(block[:, k : k + LANES] * scale).astype(BF16) for k in range(0, units, LANES)], axis=1
        )

    def cast_weights(source, send, recv, sent):
        def step(i):
            e = jnp.bitwise_xor(f, offset(i))
            load(source, i).wait()
            cast = scaled(stage[i % STAGES])

            @pl.when(i < n_fs - 1)
            def _():
                send[e] = cast

            @pl.when(i == n_fs - 1)
            def _():
                recv[pl.ds(aligned(f * rows), rows), :] = cast

            @pl.when(i + STAGES < n_fs)
            def _():
                load(source, i + STAGES).start()

            if sent is not None:
                pl.when(i > 0)(lambda: sent(jnp.bitwise_xor(f, offset(i - 1))))

        each(n_fs, step)

    def send_gate(e):
        weight_copy(gate_send, gate_recv, gate_ss, gate_rs, e, f).start()

    def send_up(e):
        weight_copy(up_send, up_recv, up_ss, up_rs, e, f).start()

    pl.semaphore_wait(barrier, total - 1)
    cast_weights(gate_in, gate_send, gate_recv, send_gate)
    for i in range(STAGES):
        load(up_in, i).start()

    for copy in small[1:3]:
        copy.wait()
    row_id = lax.broadcasted_iota(jnp.int32, (count, count), 0)
    column_id = lax.broadcasted_iota(jnp.int32, (count, count), 1)
    expert_row = lax.broadcasted_iota(jnp.int32, (n_fs, count), 0)
    first, second = expert_row == routes[0:1, :], expert_row == routes[1:2, :]
    named = first | second
    before = jnp.dot(
        jnp.where(named, 1.0, 0.0).astype(BF16),
        jnp.where(row_id < column_id, 1.0, 0.0).astype(BF16),
        preferred_element_type=F32,
    )
    before = jnp.where(named, before, -1.0)
    slot_across[...] = before
    slot[...] = before.T
    share[...] = (jnp.where(first, weight[0:1, :], 0.0) + jnp.where(second, weight[1:2, :], 0.0)).T

    def norm(i):
        at = pl.ds(aligned(i * strip, strip), strip)
        token_load(i).wait()
        values = tokens[i % 2].astype(F32)
        scale = lax.rsqrt(jnp.mean(values * values, axis=1, keepdims=True) + 1e-06)
        mine = tokens[i % 2, :, pl.ds(aligned(t * columns), columns)].astype(F32)
        normed[at, :] = (mine * scale).astype(BF16)

        @pl.when(i + 2 < count // strip)
        def _():
            token_load(i + 2).start()

    each(count // strip, norm)

    def token_copy(e, owner):
        return remote(
            outgoing.at[e, pl.ds(0, CAP)],
            incoming.at[owner, pl.ds(0, CAP), pl.ds(aligned(t * columns), columns)],
            token_ss.at[e],
            token_rs.at[owner],
            e,
            t,
        )

    slot_id = lax.broadcasted_iota(jnp.int32, (ROWS, count), 0).astype(F32)

    def dispatch(i):
        e = jnp.bitwise_xor(f, offset(i))
        pick = jnp.where(slot_id == slot_across[pl.ds(e, 1), :], 1.0, 0.0).astype(BF16)
        picked = jnp.dot(pick, normed[...], preferred_element_type=F32).astype(BF16)

        @pl.when(i < n_fs - 1)
        def _():
            outgoing[e] = picked

        @pl.when(i == n_fs - 1)
        def _():
            incoming[f, :, pl.ds(aligned(t * columns), columns)] = picked

        @pl.when(i > 0)
        def _():
            token_copy(jnp.bitwise_xor(f, offset(i - 1)), f).start()

    each(n_fs, dispatch)

    cast_weights(up_in, up_send, up_recv, None)

    def down_load(i):
        return pltpu.make_async_copy(down_in.at[i], down_stage.at[i % 2], down_load_sem.at[i % 2])

    owner = f // ratio

    def place(c, tp):
        return pl.ds(aligned(tp * columns + c * LANES), LANES)

    def down_copy(c, e, to, fs, tp):
        return remote(
            down_send.at[c, e],
            down_recv.at[pl.ds(aligned(fs % ratio * part), part), place(c, tp)],
            down_ss.at[c, e],
            down_rs.at[c, fs % ratio * n_tp + tp],
            e,
            to,
        )

    down_load(0).start()
    down_load(1).start()

    def down_cast(i):
        down_load(i).wait()
        for c in range(chunks):
            down_send[c, i] = down_stage[i % 2, :, c * LANES : (c + 1) * LANES].astype(BF16)

        @pl.when(i + 2 < n_fs)
        def _():
            down_load(i + 2).start()

    each(n_fs, down_cast)

    def send_down(c):
        def one(i):
            e = jnp.bitwise_xor(f, offset(i))
            mine = (e == f) & (owner == t)

            @pl.when(mine)
            def _():
                down_recv[pl.ds(aligned(f % ratio * part), part), place(c, t)] = down_send[c, e]

            @pl.when(jnp.logical_not(mine))
            def _():
                down_copy(c, e, owner, f, t).start()

        each(n_fs, one)

    def peers(action):
        each(n_fs - 1, lambda i: action(jnp.bitwise_xor(f, i + 1)))

    peers(lambda e: token_copy(e, e).wait_recv())
    each(n_fs - 1, lambda i: send_up(jnp.bitwise_xor(f, offset(i))))

    def span(tp):
        return incoming.at[:, pl.ds(0, CAP), pl.ds(aligned(tp * columns), columns)]

    def line(d, chip):
        other = jnp.bitwise_xor(x, d)
        return remote(
            span(chip * 2 + core), span(chip * 2 + core), line_ss.at[d - 1], line_rs.at[d - 1], f, other * 2 + core
        )

    def pair(d, on):
        chip = jnp.bitwise_xor(x, d)
        return remote(
            span(chip * 2 + on), span(chip * 2 + on), pair_ss.at[d], pair_rs.at[d], f, x * 2 + 1 - core
        )

    for d in range(1, chips):
        line(d, x).start()
    pair(0, core).start()
    for d in range(1, chips):
        line(d, jnp.bitwise_xor(x, d)).wait_recv()
        pair(d, core).start()
    for d in range(chips):
        pair(d, 1 - core).wait_recv()

    peers(lambda e: weight_copy(gate_send, gate_recv, gate_ss, gate_rs, e, e).wait_recv())
    peers(lambda e: weight_copy(up_send, up_recv, up_ss, up_rs, e, e).wait_recv())
    each(chunks, send_down)
    tile = 256
    width = incoming.shape[2]
    group = 2

    def hidden_step(i):
        g, n = i // (units // tile), i % (units // tile)
        lanes = pl.ds(aligned(n * tile, tile), tile)
        at = pl.ds(g * group, group)
        received = incoming[at].reshape(group * ROWS, width)
        gate_pre = jnp.dot(received, gate_recv[:, lanes], preferred_element_type=F32)
        up_pre = jnp.dot(received, up_recv[:, lanes], preferred_element_type=F32)
        value = gate_pre / (1.0 + jnp.exp(-gate_pre)) * up_pre
        hidden[at, :, lanes] = value.astype(BF16).reshape(group, ROWS, tile)

    each(n_fs // group * (units // tile), hidden_step)

    def far_copy(c):
        return remote(far, far_recv.at[c], far_ss.at[c], far_rs.at[c], f, x * 2 + 1 - core)

    def across_copy(c, d):
        other = jnp.bitwise_xor(x, d)
        return remote(
            near.at[c % 2, other], across_recv.at[c, d - 1], across_ss.at[c, d - 1], across_rs.at[c, d - 1],
            f, other * 2 + core,
        )

    def back_copy(c, e, owner):
        return remote(
            back_send.at[c, e, pl.ds(0, CAP)],
            back_recv.at[c, owner, pl.ds(0, CAP)],
            back_ss.at[c, e],
            back_rs.at[c, owner],
            e,
            t,
        )

    def send_back(c):
        peers(lambda e: back_copy(c, e, f).start())

    def product(c, side, store):
        taken = jnp.concatenate([down_recv[:, place(c, 2 * chip + side)] for chip in range(chips)], axis=1)

        def step(g):
            at = pl.ds(g * group, group)
            value = jnp.dot(
                hidden[at].reshape(group * ROWS, units), taken, preferred_element_type=F32
            ).astype(BF16)
            for chip in range(chips):
                store(chip, at, value[:, chip * LANES : (chip + 1) * LANES].reshape(group, ROWS, LANES))

        each(n_fs // group, step)

    def store_far(chip, at, value):
        far[chip, at] = value

    def finish(c):
        for d in range(1, chips):
            across_copy(c, d).wait_recv()

        def one(e):
            value = near[c % 2, x, e].astype(F32) + far_recv[c, x, e].astype(F32)
            for d in range(1, chips):
                value = value + across_recv[c, d - 1, e].astype(F32)
            back_send[c, e] = value.astype(BF16)

        each(n_fs, one)
        back_recv[c, f, pl.ds(0, CAP), :] = back_send[c, f, pl.ds(0, CAP), :]

    def down_chunk(c):
        def store_near(chip, at, value):
            near[c % 2, chip, at] = value

        def arrival(i):
            fs, tp = t * ratio + i // n_tp, i % n_tp

            @pl.when(jnp.logical_not((fs == f) & (tp == t)))
            def _():
                down_copy(c, f, t, fs, tp).wait_recv()

        each(ratio * n_tp, arrival)

        @pl.when(c == chunks - 1)
        def _():
            each(chunks - 2, send_back)

        product(c, 1 - core, store_far)
        far_copy(c).start()

        @pl.when(c > 1)
        def _():
            for d in range(1, chips):
                across_copy(c - 2, d).wait_send()

        product(c, core, store_near)
        far_copy(c).wait()
        for d in range(1, chips):
            other = jnp.bitwise_xor(x, d)

            def add(e):
                total = near[c % 2, other, e].astype(F32) + far_recv[c, other, e].astype(F32)
                near[c % 2, other, e] = total.astype(BF16)

            each(n_fs, add)
            across_copy(c, d).start()

        @pl.when(c > 0)
        def _():
            finish(c - 1)

    each(chunks, down_chunk)
    send_back(chunks - 2)
    finish(chunks - 1)
    send_back(chunks - 1)
    for c in range(chunks - 2, chunks):
        for d in range(1, chips):
            across_copy(c, d).wait_send()

    lane_id = lax.broadcasted_iota(jnp.int32, (count, DEPTH), 1).astype(F32)

    def combine(c):
        peers(lambda e: back_copy(c, e, e).wait_recv())
        value = jnp.zeros((count, LANES), F32)
        for e in range(n_fs):
            pick = jnp.where(lane_id == slot[:, e : e + 1], 1.0, 0.0).astype(BF16)
            value = value + share[:, e : e + 1] * jnp.dot(pick, back_recv[c, e], preferred_element_type=F32)
        result[:, pl.ds(aligned(c * LANES), LANES)] = value.astype(BF16)

    each(chunks, combine)

    peers(lambda e: weight_copy(gate_send, gate_recv, gate_ss, gate_rs, e, f).wait_send())
    peers(lambda e: weight_copy(up_send, up_recv, up_ss, up_rs, e, f).wait_send())
    peers(lambda e: token_copy(e, f).wait_send())
    for d in range(1, chips):
        line(d, x).wait_send()
    for d in range(chips):
        pair(d, core).wait_send()

    def drain(c):
        def one(e):
            @pl.when(jnp.logical_not((e == f) & (owner == t)))
            def _():
                down_copy(c, e, owner, f, t).wait_send()

        each(n_fs, one)
        peers(lambda e: back_copy(c, e, f).wait_send())

    each(chunks, drain)


def body(tokens, routes, route_weight, norm_gain, gate_master, up_master, down_master):
    n_fs, n_tp = lax.axis_size("fs"), lax.axis_size("tp")
    count, width = tokens.shape
    experts, rows, units = gate_master.shape
    part, columns = down_master.shape[1:]
    chips, chunks, ratio = n_tp // 2, columns // LANES, n_fs // n_tp
    assert experts == n_fs
    dma = pltpu.SemaphoreType.DMA
    lines = max(1, chips - 1)
    scratch = [
        pltpu.VMEM((n_fs, rows, units), BF16),
        pltpu.VMEM((n_fs, rows, units), BF16),
        pltpu.VMEM((chunks, n_fs, part, LANES), BF16),
        pltpu.VMEM((STAGES, rows, units), F32),
        pltpu.VMEM((2, part, columns), F32),
        pltpu.VMEM((2, count // 8, width), BF16),
        pltpu.VMEM((count, columns), BF16),
        pltpu.VMEM((n_fs, ROWS, columns), BF16),
        pltpu.VMEM((n_fs, ROWS, width), BF16),
        pltpu.VMEM((n_fs, ROWS, units), BF16),
        pltpu.VMEM((chips, n_fs, ROWS, LANES), BF16),
        pltpu.VMEM((chunks, chips, n_fs, ROWS, LANES), BF16),
        pltpu.VMEM((2, chips, n_fs, ROWS, LANES), BF16),
        pltpu.VMEM((chunks, lines, n_fs, ROWS, LANES), BF16),
        pltpu.VMEM((chunks, n_fs, ROWS, LANES), BF16),
        pltpu.VMEM((chunks, n_fs, DEPTH, LANES), BF16),
        pltpu.VMEM((1, rows), F32),
        pltpu.VMEM((rows, LANES), F32),
        pltpu.VMEM((2, count), jnp.int32),
        pltpu.VMEM((2, count), F32),
        pltpu.VMEM((n_fs, count), F32),
        pltpu.VMEM((count, n_fs), F32),
        pltpu.VMEM((count, n_fs), F32),
        dma((STAGES,)), dma((2,)), dma((3,)), dma((2,)),
        dma((n_fs,)), dma((n_fs,)), dma((n_fs,)), dma((n_fs,)), dma((n_fs,)), dma((n_fs,)),
        dma((chunks, n_fs)), dma((chunks, ratio * n_tp)),
        dma((lines,)), dma((lines,)), dma((chips,)), dma((chips,)),
        dma((chunks,)), dma((chunks,)), dma((chunks, lines)), dma((chunks, lines)),
        dma((chunks, n_fs)), dma((chunks, n_fs)),
    ]
    shapes = (
        (n_fs * rows, units), (n_fs * rows, units), (ratio * part, n_tp * columns), (count, columns)
    )
    kept = sum(2 * a * b for a, b in shapes)
    anywhere = pl.BlockSpec(memory_space=pl.ANY)
    return pl.pallas_call(
        functools.partial(kernel, n_fs, n_tp),
        out_shape=tuple(pltpu.VMEM(shape, BF16) for shape in shapes),
        in_specs=[anywhere] * 7,
        out_specs=(pl.BlockSpec(memory_space=pltpu.VMEM),) * 4,
        scratch_shapes=scratch,
        compiler_params=pltpu.CompilerParams(
            collective_id=0, has_side_effects=True, vmem_limit_bytes=VMEM - kept
        ),
        name="layer",
    )(routes.T, route_weight.T, norm_gain[None], tokens, gate_master, up_master, down_master)


def solution(mesh):
    placed = (
        P("fs", None),
        P("fs", None),
        P("fs", None),
        P("fs"),
        P(None, "fs", "tp"),
        P(None, "fs", "tp"),
        P(None, "fs", "tp"),
    )

    def step(*args):
        gate, up, down, out = body(*args)
        return gate[None], up[None], down[None], out

    return jax.shard_map(
        step,
        mesh=mesh,
        in_specs=placed,
        out_specs=(P("fs", None, "tp"), P("fs", None, "tp"), P("fs", "tp", None), P("fs", "tp")),
        check_vma=False,
    )
```

```python
import functools

import jax
import jax.numpy as jnp
from jax import lax
from jax.experimental import pallas as pl
from jax.experimental.pallas import tpu as pltpu
from jax.sharding import PartitionSpec as P

CAP = 216
ROWS = 224
DEPTH = 256
LANES = 128
STAGES = 3
VMEM = 67 * 1000 * 1000
MESH = pl.DeviceIdType.MESH
F32, BF16 = jnp.float32, jnp.bfloat16


def aligned(value, step=LANES):
    return pl.multiple_of(value, step)


def weighted(slot, share, rows_of):
    count, n_fs = slot.shape
    lane_id = lax.broadcasted_iota(jnp.int32, (count, DEPTH), 1).astype(F32)
    value = jnp.zeros((count, LANES), F32)
    for e in range(n_fs):
        pick = jnp.where(lane_id == slot[:, e : e + 1], 1.0, 0.0).astype(BF16)
        value = value + share[:, e : e + 1] * jnp.dot(pick, rows_of(e), preferred_element_type=F32)
    return value.astype(BF16)


def store_kernel(gate, up, down, result, back, slot, share, gate_out, up_out, down_out, layer_out, last, sem):
    early = result.shape[1] - LANES
    copies = [
        pltpu.make_async_copy(gate, gate_out, sem.at[0]),
        pltpu.make_async_copy(up, up_out, sem.at[1]),
        pltpu.make_async_copy(down, down_out, sem.at[2]),
        pltpu.make_async_copy(result.at[:, pl.ds(0, early)], layer_out.at[:, pl.ds(0, early)], sem.at[3]),
    ]
    for copy in copies:
        copy.start()
    chunk = back.shape[0] - 1
    last[...] = weighted(slot, share, lambda e: back[chunk, e])
    copies.append(pltpu.make_async_copy(last, layer_out.at[:, pl.ds(early, LANES)], sem.at[4]))
    copies[-1].start()
    for copy in copies:
        copy.wait()


def kernel(
    n_fs, n_tp, routes_in, weight_in, gain_in, tokens_in, gate_in, up_in, down_in,
    gate_recv, up_recv, down_recv, result, back_recv, slot, share,
    gate_send, up_send, down_send, stage, down_stage,
    tokens, normed, outgoing, incoming, hidden, far, far_recv, near, across_recv,
    back_send, gain_row, gain, routes, weight, slot_across,
    load_sem, down_load_sem, small_sem, token_load_sem, gate_ss, gate_rs, up_ss, up_rs, token_ss, token_rs,
    down_ss, down_rs, line_ss, line_rs, pair_ss, pair_rs, far_ss, far_rs, across_ss, across_rs,
    back_ss, back_rs,
):
    f, t = lax.axis_index("fs"), lax.axis_index("tp")
    core, x = t % 2, t // 2
    chips = n_tp // 2
    ratio = n_fs // n_tp
    rows, units = gate_send.shape[1:]
    part = down_stage.shape[1]
    columns = down_stage.shape[2]
    chunks = columns // LANES
    half = n_fs // 2

    def remote(src, dst, ss, rs, fs, tp):
        return pltpu.make_async_remote_copy(
            src_ref=src, dst_ref=dst, send_sem=ss, recv_sem=rs,
            device_id={"fs": fs, "tp": tp}, device_id_type=MESH,
        )

    def each(n, action):
        def step(i, carry):
            action(i)
            return carry

        lax.fori_loop(0, n, step, 0)

    def offset(i):
        return jnp.where(i < half, i + half, jnp.where(i == n_fs - 1, 0, i - half + 1))

    small = [
        pltpu.make_async_copy(gain_in, gain_row, small_sem.at[0]),
        pltpu.make_async_copy(routes_in, routes, small_sem.at[1]),
        pltpu.make_async_copy(weight_in, weight, small_sem.at[2]),
    ]
    small[0].start()

    def load(source, i):
        return pltpu.make_async_copy(
            source.at[jnp.bitwise_xor(f, offset(i))], stage.at[i % STAGES], load_sem.at[i % STAGES]
        )

    for i in range(STAGES):
        load(gate_in, i).start()
    for copy in small[1:]:
        copy.start()
    strip = tokens.shape[1]
    count = normed.shape[0]

    def token_load(i):
        return pltpu.make_async_copy(
            tokens_in.at[pl.ds(aligned(i * strip, strip), strip)], tokens.at[i % 2], token_load_sem.at[i % 2]
        )

    token_load(0).start()
    token_load(1).start()

    barrier = pltpu.get_barrier_semaphore()
    total = n_fs * n_tp
    me = f * n_tp + t

    def greet(i):
        other = (me + i + 1) % total
        pl.semaphore_signal(
            barrier, inc=1, device_id={"fs": other // n_tp, "tp": other % n_tp}, device_id_type=MESH
        )

    each(total - 1, greet)

    back_recv[:, :, CAP:, :] = jnp.zeros((chunks, n_fs, DEPTH - CAP, LANES), BF16)

    small[0].wait()
    same = lax.broadcasted_iota(jnp.int32, (rows, rows), 0) == lax.broadcasted_iota(jnp.int32, (rows, rows), 1)
    column = jnp.sum(jnp.where(same, gain_row[...], 0.0), axis=1, keepdims=True)
    gain[...] = jnp.broadcast_to(column, (rows, LANES))

    def weight_copy(send, recv, ss, rs, e, owner):
        return remote(
            send.at[e], recv.at[pl.ds(aligned(owner * rows), rows)], ss.at[e], rs.at[owner], e, t
        )

    def scaled(block):
        scale = gain[...]
        return jnp.concatenate(
            [(block[:, k : k + LANES] * scale).astype(BF16) for k in range(0, units, LANES)], axis=1
        )

    def cast_weights(source, send, recv, sent):
        def step(i):
            e = jnp.bitwise_xor(f, offset(i))
            load(source, i).wait()
            cast = scaled(stage[i % STAGES])

            @pl.when(i < n_fs - 1)
            def _():
                send[e] = cast

            @pl.when(i == n_fs - 1)
            def _():
                recv[pl.ds(aligned(f * rows), rows), :] = cast

            @pl.when(i + STAGES < n_fs)
            def _():
                load(source, i + STAGES).start()

        def send_step(i):
            step(i)
            sent(jnp.bitwise_xor(f, offset(i - 1)))

        if sent is None:
            each(n_fs, step)
        else:
            each(2, step)
            pl.semaphore_wait(barrier, total - 1)
            sent(jnp.bitwise_xor(f, offset(0)))
            each(n_fs - 2, lambda i: send_step(i + 2))

    def send_gate(e):
        weight_copy(gate_send, gate_recv, gate_ss, gate_rs, e, f).start()

    def send_up(e):
        weight_copy(up_send, up_recv, up_ss, up_rs, e, f).start()

    cast_weights(gate_in, gate_send, gate_recv, send_gate)
    for i in range(STAGES):
        load(up_in, i).start()

    for copy in small[1:3]:
        copy.wait()
    row_id = lax.broadcasted_iota(jnp.int32, (count, count), 0)
    column_id = lax.broadcasted_iota(jnp.int32, (count, count), 1)
    expert_row = lax.broadcasted_iota(jnp.int32, (n_fs, count), 0)
    first, second = expert_row == routes[0:1, :], expert_row == routes[1:2, :]
    named = first | second
    before = jnp.dot(
        jnp.where(named, 1.0, 0.0).astype(BF16),
        jnp.where(row_id < column_id, 1.0, 0.0).astype(BF16),
        preferred_element_type=F32,
    )
    before = jnp.where(named, before, -1.0)
    slot_across[...] = before
    slot[...] = before.T
    share[...] = (jnp.where(first, weight[0:1, :], 0.0) + jnp.where(second, weight[1:2, :], 0.0)).T

    def norm(i):
        at = pl.ds(aligned(i * strip, strip), strip)
        token_load(i).wait()
        values = tokens[i % 2].astype(F32)
        scale = lax.rsqrt(jnp.mean(values * values, axis=1, keepdims=True) + 1e-06)
        mine = tokens[i % 2, :, pl.ds(aligned(t * columns), columns)].astype(F32)
        normed[at, :] = (mine * scale).astype(BF16)

        @pl.when(i + 2 < count // strip)
        def _():
            token_load(i + 2).start()

    each(count // strip, norm)

    def token_copy(e, owner):
        return remote(
            outgoing.at[e, pl.ds(0, CAP)],
            incoming.at[owner, pl.ds(0, CAP), pl.ds(aligned(t * columns), columns)],
            token_ss.at[e],
            token_rs.at[owner],
            e,
            t,
        )

    slot_id = lax.broadcasted_iota(jnp.int32, (ROWS, count), 0).astype(F32)

    def dispatch(i):
        e = jnp.bitwise_xor(f, offset(i))
        pick = jnp.where(slot_id == slot_across[pl.ds(e, 1), :], 1.0, 0.0).astype(BF16)
        picked = jnp.dot(pick, normed[...], preferred_element_type=F32).astype(BF16)

        @pl.when(i < n_fs - 1)
        def _():
            outgoing[e] = picked

        @pl.when(i == n_fs - 1)
        def _():
            incoming[f, :, pl.ds(aligned(t * columns), columns)] = picked

        @pl.when(i > 0)
        def _():
            token_copy(jnp.bitwise_xor(f, offset(i - 1)), f).start()

    each(n_fs, dispatch)

    cast_weights(up_in, up_send, up_recv, None)

    def down_load(i):
        return pltpu.make_async_copy(down_in.at[i], down_stage.at[i % 2], down_load_sem.at[i % 2])

    owner = f // ratio

    def place(c, tp):
        return pl.ds(aligned(tp * columns + c * LANES), LANES)

    def down_copy(c, e, to, fs, tp):
        return remote(
            down_send.at[c, e],
            down_recv.at[pl.ds(aligned(fs % ratio * part), part), place(c, tp)],
            down_ss.at[c, e],
            down_rs.at[c, fs % ratio * n_tp + tp],
            e,
            to,
        )

    down_load(0).start()
    down_load(1).start()

    def down_cast(i):
        down_load(i).wait()
        for c in range(chunks):
            down_send[c, i] = down_stage[i % 2, :, c * LANES : (c + 1) * LANES].astype(BF16)

        @pl.when(i + 2 < n_fs)
        def _():
            down_load(i + 2).start()

    each(n_fs, down_cast)

    def send_down(c):
        def one(i):
            e = jnp.bitwise_xor(f, offset(i))
            mine = (e == f) & (owner == t)

            @pl.when(mine)
            def _():
                down_recv[pl.ds(aligned(f % ratio * part), part), place(c, t)] = down_send[c, e]

            @pl.when(jnp.logical_not(mine))
            def _():
                down_copy(c, e, owner, f, t).start()

        each(n_fs, one)

    def peers(action):
        each(n_fs - 1, lambda i: action(jnp.bitwise_xor(f, i + 1)))

    peers(lambda e: token_copy(e, e).wait_recv())
    each(n_fs - 1, lambda i: send_up(jnp.bitwise_xor(f, offset(i))))

    def span(tp):
        return incoming.at[:, pl.ds(0, CAP), pl.ds(aligned(tp * columns), columns)]

    def line(d, chip):
        other = jnp.bitwise_xor(x, d)
        return remote(
            span(chip * 2 + core), span(chip * 2 + core), line_ss.at[d - 1], line_rs.at[d - 1], f, other * 2 + core
        )

    def pair(d, on):
        chip = jnp.bitwise_xor(x, d)
        return remote(
            span(chip * 2 + on), span(chip * 2 + on), pair_ss.at[d], pair_rs.at[d], f, x * 2 + 1 - core
        )

    for d in range(1, chips):
        line(d, x).start()
    pair(0, core).start()
    for d in range(1, chips):
        line(d, jnp.bitwise_xor(x, d)).wait_recv()
        pair(d, core).start()
    for d in range(chips):
        pair(d, 1 - core).wait_recv()

    peers(lambda e: weight_copy(gate_send, gate_recv, gate_ss, gate_rs, e, e).wait_recv())
    peers(lambda e: weight_copy(up_send, up_recv, up_ss, up_rs, e, e).wait_recv())
    each(chunks, send_down)
    tile = 256
    width = incoming.shape[2]
    group = 2

    def hidden_step(i):
        g, n = i // (units // tile), i % (units // tile)
        lanes = pl.ds(aligned(n * tile, tile), tile)
        at = pl.ds(g * group, group)
        received = incoming[at].reshape(group * ROWS, width)
        gate_pre = jnp.dot(received, gate_recv[:, lanes], preferred_element_type=F32)
        up_pre = jnp.dot(received, up_recv[:, lanes], preferred_element_type=F32)
        value = gate_pre / (1.0 + jnp.exp(-gate_pre)) * up_pre
        hidden[at, :, lanes] = value.astype(BF16).reshape(group, ROWS, tile)

    each(n_fs // group * (units // tile), hidden_step)

    def far_copy(c):
        return remote(far, far_recv.at[c], far_ss.at[c], far_rs.at[c], f, x * 2 + 1 - core)

    def across_copy(c, d):
        other = jnp.bitwise_xor(x, d)
        return remote(
            near.at[c % 2, other], across_recv.at[c, d - 1], across_ss.at[c, d - 1], across_rs.at[c, d - 1],
            f, other * 2 + core,
        )

    def back_copy(c, e, owner):
        return remote(
            back_send.at[c, e, pl.ds(0, CAP)],
            back_recv.at[c, owner, pl.ds(0, CAP)],
            back_ss.at[c, e],
            back_rs.at[c, owner],
            e,
            t,
        )

    def send_back(c):
        peers(lambda e: back_copy(c, e, f).start())

    def product(c, side, store):
        taken = jnp.concatenate([down_recv[:, place(c, 2 * chip + side)] for chip in range(chips)], axis=1)

        def step(g):
            at = pl.ds(g * group, group)
            value = jnp.dot(
                hidden[at].reshape(group * ROWS, units), taken, preferred_element_type=F32
            ).astype(BF16)
            for chip in range(chips):
                store(chip, at, value[:, chip * LANES : (chip + 1) * LANES].reshape(group, ROWS, LANES))

        each(n_fs // group, step)

    def store_far(chip, at, value):
        far[chip, at] = value

    def finish(c):
        for d in range(1, chips):
            across_copy(c, d).wait_recv()

        def one(e):
            value = near[c % 2, x, e].astype(F32) + far_recv[c, x, e].astype(F32)
            for d in range(1, chips):
                value = value + across_recv[c, d - 1, e].astype(F32)
            back_send[c, e] = value.astype(BF16)

        each(n_fs, one)
        back_recv[c, f, pl.ds(0, CAP), :] = back_send[c, f, pl.ds(0, CAP), :]

    def down_chunk(c):
        def store_near(chip, at, value):
            near[c % 2, chip, at] = value

        def arrival(i):
            fs, tp = t * ratio + i // n_tp, i % n_tp

            @pl.when(jnp.logical_not((fs == f) & (tp == t)))
            def _():
                down_copy(c, f, t, fs, tp).wait_recv()

        each(ratio * n_tp, arrival)

        @pl.when(c == chunks - 1)
        def _():
            each(chunks - 2, send_back)

        product(c, 1 - core, store_far)
        far_copy(c).start()

        @pl.when(c > 1)
        def _():
            for d in range(1, chips):
                across_copy(c - 2, d).wait_send()

        product(c, core, store_near)
        far_copy(c).wait()
        for d in range(1, chips):
            other = jnp.bitwise_xor(x, d)

            def add(e):
                total = near[c % 2, other, e].astype(F32) + far_recv[c, other, e].astype(F32)
                near[c % 2, other, e] = total.astype(BF16)

            each(n_fs, add)
            across_copy(c, d).start()

        @pl.when(c > 0)
        def _():
            finish(c - 1)

    each(chunks, down_chunk)
    send_back(chunks - 2)
    finish(chunks - 1)
    send_back(chunks - 1)
    for c in range(chunks - 2, chunks):
        for d in range(1, chips):
            across_copy(c, d).wait_send()

    def combine(c):
        peers(lambda e: back_copy(c, e, e).wait_recv())
        result[:, pl.ds(aligned(c * LANES), LANES)] = weighted(slot, share, lambda e: back_recv[c, e])

    each(chunks - 1, combine)
    peers(lambda e: back_copy(chunks - 1, e, e).wait_recv())

    peers(lambda e: weight_copy(gate_send, gate_recv, gate_ss, gate_rs, e, f).wait_send())
    peers(lambda e: weight_copy(up_send, up_recv, up_ss, up_rs, e, f).wait_send())
    peers(lambda e: token_copy(e, f).wait_send())
    for d in range(1, chips):
        line(d, x).wait_send()
    for d in range(chips):
        pair(d, core).wait_send()

    def drain(c):
        def one(e):
            @pl.when(jnp.logical_not((e == f) & (owner == t)))
            def _():
                down_copy(c, e, owner, f, t).wait_send()

        each(n_fs, one)
        peers(lambda e: back_copy(c, e, f).wait_send())

    each(chunks, drain)


def body(tokens, routes, route_weight, norm_gain, gate_master, up_master, down_master):
    n_fs, n_tp = lax.axis_size("fs"), lax.axis_size("tp")
    count, width = tokens.shape
    experts, rows, units = gate_master.shape
    part, columns = down_master.shape[1:]
    chips, chunks, ratio = n_tp // 2, columns // LANES, n_fs // n_tp
    assert experts == n_fs
    dma = pltpu.SemaphoreType.DMA
    lines = max(1, chips - 1)
    scratch = [
        pltpu.VMEM((n_fs, rows, units), BF16),
        pltpu.VMEM((n_fs, rows, units), BF16),
        pltpu.VMEM((chunks, n_fs, part, LANES), BF16),
        pltpu.VMEM((STAGES, rows, units), F32),
        pltpu.VMEM((2, part, columns), F32),
        pltpu.VMEM((2, count // 8, width), BF16),
        pltpu.VMEM((count, columns), BF16),
        pltpu.VMEM((n_fs, ROWS, columns), BF16),
        pltpu.VMEM((n_fs, ROWS, width), BF16),
        pltpu.VMEM((n_fs, ROWS, units), BF16),
        pltpu.VMEM((chips, n_fs, ROWS, LANES), BF16),
        pltpu.VMEM((chunks, chips, n_fs, ROWS, LANES), BF16),
        pltpu.VMEM((2, chips, n_fs, ROWS, LANES), BF16),
        pltpu.VMEM((chunks, lines, n_fs, ROWS, LANES), BF16),
        pltpu.VMEM((chunks, n_fs, ROWS, LANES), BF16),
        pltpu.VMEM((1, rows), F32),
        pltpu.VMEM((rows, LANES), F32),
        pltpu.VMEM((2, count), jnp.int32),
        pltpu.VMEM((2, count), F32),
        pltpu.VMEM((n_fs, count), F32),
        dma((STAGES,)), dma((2,)), dma((3,)), dma((2,)),
        dma((n_fs,)), dma((n_fs,)), dma((n_fs,)), dma((n_fs,)), dma((n_fs,)), dma((n_fs,)),
        dma((chunks, n_fs)), dma((chunks, ratio * n_tp)),
        dma((lines,)), dma((lines,)), dma((chips,)), dma((chips,)),
        dma((chunks,)), dma((chunks,)), dma((chunks, lines)), dma((chunks, lines)),
        dma((chunks, n_fs)), dma((chunks, n_fs)),
    ]
    shapes = (
        (n_fs * rows, units), (n_fs * rows, units), (ratio * part, n_tp * columns), (count, columns)
    )
    kept = sum(2 * a * b for a, b in shapes) + 2 * chunks * n_fs * DEPTH * LANES + 8 * count * LANES
    anywhere, vector = pl.BlockSpec(memory_space=pl.ANY), pl.BlockSpec(memory_space=pltpu.VMEM)
    held = pl.pallas_call(
        functools.partial(kernel, n_fs, n_tp),
        out_shape=(
            *(pltpu.VMEM(shape, BF16) for shape in shapes),
            pltpu.VMEM((chunks, n_fs, DEPTH, LANES), BF16),
            pltpu.VMEM((count, n_fs), F32),
            pltpu.VMEM((count, n_fs), F32),
        ),
        in_specs=[anywhere] * 7,
        out_specs=(vector,) * 7,
        scratch_shapes=scratch,
        compiler_params=pltpu.CompilerParams(
            collective_id=0, has_side_effects=True, vmem_limit_bytes=VMEM - kept
        ),
        name="layer",
    )(routes.T, route_weight.T, norm_gain[None], tokens, gate_master, up_master, down_master)
    return pl.pallas_call(
        store_kernel,
        out_shape=tuple(jax.ShapeDtypeStruct(shape, BF16) for shape in shapes),
        in_specs=[vector] * 7,
        out_specs=(anywhere,) * 4,
        scratch_shapes=[pltpu.VMEM((count, LANES), BF16), dma((5,))],
        compiler_params=pltpu.CompilerParams(vmem_limit_bytes=16 * 1000 * 1000),
        name="store",
    )(*(pltpu.with_memory_space_constraint(value, pltpu.VMEM) for value in held))


def solution(mesh):
    placed = (
        P("fs", None),
        P("fs", None),
        P("fs", None),
        P("fs"),
        P(None, "fs", "tp"),
        P(None, "fs", "tp"),
        P(None, "fs", "tp"),
    )

    def step(*args):
        gate, up, down, out = body(*args)
        return gate[None], up[None], down[None], out

    return jax.shard_map(
        step,
        mesh=mesh,
        in_specs=placed,
        out_specs=(P("fs", None, "tp"), P("fs", None, "tp"), P("fs", "tp", None), P("fs", "tp")),
        check_vma=False,
    )
```

```python
import functools

import jax
import jax.numpy as jnp
from jax import lax
from jax.experimental import pallas as pl
from jax.experimental.pallas import tpu as pltpu
from jax.sharding import PartitionSpec as P

CAP = 216
ROWS = 224
DEPTH = 256
LANES = 128
STAGES = 3
VMEM = 67 * 1000 * 1000
MESH = pl.DeviceIdType.MESH
F32, BF16 = jnp.float32, jnp.bfloat16


def aligned(value, step=LANES):
    return pl.multiple_of(value, step)


def weighted(slot, share, rows_of):
    count, n_fs = slot.shape
    lane_id = lax.broadcasted_iota(jnp.int32, (count, DEPTH), 1).astype(F32)
    value = jnp.zeros((count, LANES), F32)
    for e in range(n_fs):
        pick = jnp.where(lane_id == slot[:, e : e + 1], 1.0, 0.0).astype(BF16)
        value = value + share[:, e : e + 1] * jnp.dot(pick, rows_of(e), preferred_element_type=F32)
    return value.astype(BF16)


def store_kernel(gate, up, down, result, back, slot, share, gate_out, up_out, down_out, layer_out, last, sem):
    early = result.shape[1] - LANES
    copies = [
        pltpu.make_async_copy(gate, gate_out, sem.at[0]),
        pltpu.make_async_copy(up, up_out, sem.at[1]),
        pltpu.make_async_copy(down, down_out, sem.at[2]),
        pltpu.make_async_copy(result.at[:, pl.ds(0, early)], layer_out.at[:, pl.ds(0, early)], sem.at[3]),
    ]
    for copy in copies:
        copy.start()
    chunk = back.shape[0] - 1
    last[...] = weighted(slot, share, lambda e: back[chunk, e])
    copies.append(pltpu.make_async_copy(last, layer_out.at[:, pl.ds(early, LANES)], sem.at[4]))
    copies[-1].start()
    for copy in copies:
        copy.wait()


def kernel(
    n_fs, n_tp, routes_in, weight_in, gain_in, tokens_in, gate_in, up_in, down_in,
    gate_recv, up_recv, down_recv, result, back_recv, slot, share,
    gate_send, up_send, down_send, stage, down_stage,
    tokens, normed, outgoing, incoming, hidden, far, far_recv, near, across_recv,
    back_send, gain_row, gain, routes, weight, slot_across,
    load_sem, down_load_sem, small_sem, token_load_sem, gate_ss, gate_rs, up_ss, up_rs, token_ss, token_rs,
    down_ss, down_rs, line_ss, line_rs, pair_ss, pair_rs, far_ss, far_rs, across_ss, across_rs,
    back_ss, back_rs,
):
    f, t = lax.axis_index("fs"), lax.axis_index("tp")
    core, x = t % 2, t // 2
    chips = n_tp // 2
    ratio = n_fs // n_tp
    rows, units = gate_send.shape[1:]
    part = down_stage.shape[1]
    columns = down_stage.shape[2]
    chunks = columns // LANES
    half = n_fs // 2

    def remote(src, dst, ss, rs, fs, tp):
        return pltpu.make_async_remote_copy(
            src_ref=src, dst_ref=dst, send_sem=ss, recv_sem=rs,
            device_id={"fs": fs, "tp": tp}, device_id_type=MESH,
        )

    def each(n, action):
        def step(i, carry):
            action(i)
            return carry

        lax.fori_loop(0, n, step, 0)

    def offset(i):
        return jnp.where(i < half, i + half, jnp.where(i == n_fs - 1, 0, i - half + 1))

    small = [
        pltpu.make_async_copy(gain_in, gain_row, small_sem.at[0]),
        pltpu.make_async_copy(routes_in, routes, small_sem.at[1]),
        pltpu.make_async_copy(weight_in, weight, small_sem.at[2]),
    ]
    small[0].start()

    def load(source, i):
        return pltpu.make_async_copy(
            source.at[jnp.bitwise_xor(f, offset(i))], stage.at[i % STAGES], load_sem.at[i % STAGES]
        )

    for i in range(STAGES):
        load(gate_in, i).start()
    for copy in small[1:]:
        copy.start()
    strip = tokens.shape[1]
    count = normed.shape[0]

    def token_load(i):
        return pltpu.make_async_copy(
            tokens_in.at[pl.ds(aligned(i * strip, strip), strip)], tokens.at[i % 2], token_load_sem.at[i % 2]
        )

    token_load(0).start()
    token_load(1).start()

    barrier = pltpu.get_barrier_semaphore()
    total = n_fs * n_tp
    me = f * n_tp + t

    def greet(i):
        other = (me + i + 1) % total
        pl.semaphore_signal(
            barrier, inc=1, device_id={"fs": other // n_tp, "tp": other % n_tp}, device_id_type=MESH
        )

    each(total - 1, greet)

    back_recv[:, :, CAP:, :] = jnp.zeros((chunks, n_fs, DEPTH - CAP, LANES), BF16)

    small[0].wait()
    same = lax.broadcasted_iota(jnp.int32, (rows, rows), 0) == lax.broadcasted_iota(jnp.int32, (rows, rows), 1)
    column = jnp.sum(jnp.where(same, gain_row[...], 0.0), axis=1, keepdims=True)
    gain[...] = jnp.broadcast_to(column, (rows, LANES))

    def weight_copy(send, recv, ss, rs, e, owner):
        return remote(
            send.at[e], recv.at[pl.ds(aligned(owner * rows), rows)], ss.at[e], rs.at[owner], e, t
        )

    def scaled(block):
        scale = gain[...]
        return jnp.concatenate(
            [(block[:, k : k + LANES] * scale).astype(BF16) for k in range(0, units, LANES)], axis=1
        )

    def cast_weights(source, send, recv, sent):
        def step(i):
            e = jnp.bitwise_xor(f, offset(i))
            load(source, i).wait()
            cast = scaled(stage[i % STAGES])

            @pl.when(i < n_fs - 1)
            def _():
                send[e] = cast

            @pl.when(i == n_fs - 1)
            def _():
                recv[pl.ds(aligned(f * rows), rows), :] = cast

            @pl.when(i + STAGES < n_fs)
            def _():
                load(source, i + STAGES).start()

        def send_step(i):
            step(i)
            sent(jnp.bitwise_xor(f, offset(i - 1)))

        if sent is None:
            each(n_fs, step)
        else:
            each(2, step)
            pl.semaphore_wait(barrier, total - 1)
            sent(jnp.bitwise_xor(f, offset(0)))
            each(n_fs - 2, lambda i: send_step(i + 2))

    def send_gate(e):
        weight_copy(gate_send, gate_recv, gate_ss, gate_rs, e, f).start()

    def send_up(e):
        weight_copy(up_send, up_recv, up_ss, up_rs, e, f).start()

    cast_weights(gate_in, gate_send, gate_recv, send_gate)
    for i in range(STAGES):
        load(up_in, i).start()

    for copy in small[1:3]:
        copy.wait()
    row_id = lax.broadcasted_iota(jnp.int32, (count, count), 0)
    column_id = lax.broadcasted_iota(jnp.int32, (count, count), 1)
    expert_row = lax.broadcasted_iota(jnp.int32, (n_fs, count), 0)
    first, second = expert_row == routes[0:1, :], expert_row == routes[1:2, :]
    named = first | second
    before = jnp.dot(
        jnp.where(named, 1.0, 0.0).astype(BF16),
        jnp.where(row_id < column_id, 1.0, 0.0).astype(BF16),
        preferred_element_type=F32,
    )
    before = jnp.where(named, before, -1.0)
    slot_across[...] = before
    slot[...] = before.T
    share[...] = (jnp.where(first, weight[0:1, :], 0.0) + jnp.where(second, weight[1:2, :], 0.0)).T

    def norm(i):
        at = pl.ds(aligned(i * strip, strip), strip)
        token_load(i).wait()
        values = tokens[i % 2].astype(F32)
        scale = lax.rsqrt(jnp.mean(values * values, axis=1, keepdims=True) + 1e-06)
        mine = tokens[i % 2, :, pl.ds(aligned(t * columns), columns)].astype(F32)
        normed[at, :] = (mine * scale).astype(BF16)

        @pl.when(i + 2 < count // strip)
        def _():
            token_load(i + 2).start()

    each(count // strip, norm)

    def token_copy(e, owner):
        return remote(
            outgoing.at[e, pl.ds(0, CAP)],
            incoming.at[owner, pl.ds(0, CAP), pl.ds(aligned(t * columns), columns)],
            token_ss.at[e],
            token_rs.at[owner],
            e,
            t,
        )

    slot_id = lax.broadcasted_iota(jnp.int32, (ROWS, count), 0).astype(F32)

    def dispatch(i):
        e = jnp.bitwise_xor(f, offset(i))
        pick = jnp.where(slot_id == slot_across[pl.ds(e, 1), :], 1.0, 0.0).astype(BF16)
        picked = jnp.dot(pick, normed[...], preferred_element_type=F32).astype(BF16)

        @pl.when(i < n_fs - 1)
        def _():
            outgoing[e] = picked

        @pl.when(i == n_fs - 1)
        def _():
            incoming[f, :, pl.ds(aligned(t * columns), columns)] = picked

        @pl.when(i > 0)
        def _():
            token_copy(jnp.bitwise_xor(f, offset(i - 1)), f).start()

    each(n_fs, dispatch)

    cast_weights(up_in, up_send, up_recv, None)

    def down_load(i):
        return pltpu.make_async_copy(down_in.at[i], down_stage.at[i % 2], down_load_sem.at[i % 2])

    owner = f // ratio

    def place(c, tp):
        return pl.ds(aligned(tp * columns + c * LANES), LANES)

    def down_copy(c, e, to, fs, tp):
        return remote(
            down_send.at[c, e],
            down_recv.at[pl.ds(aligned(fs % ratio * part), part), place(c, tp)],
            down_ss.at[c, e],
            down_rs.at[c, fs % ratio * n_tp + tp],
            e,
            to,
        )

    down_load(0).start()
    down_load(1).start()

    def down_cast(i):
        down_load(i).wait()
        for c in range(chunks):
            down_send[c, i] = down_stage[i % 2, :, c * LANES : (c + 1) * LANES].astype(BF16)

        @pl.when(i + 2 < n_fs)
        def _():
            down_load(i + 2).start()

    each(n_fs, down_cast)

    def send_down(c):
        def one(i):
            e = jnp.bitwise_xor(f, offset(i))
            mine = (e == f) & (owner == t)

            @pl.when(mine)
            def _():
                down_recv[pl.ds(aligned(f % ratio * part), part), place(c, t)] = down_send[c, e]

            @pl.when(jnp.logical_not(mine))
            def _():
                down_copy(c, e, owner, f, t).start()

        each(n_fs, one)

    def peers(action):
        each(n_fs - 1, lambda i: action(jnp.bitwise_xor(f, i + 1)))

    peers(lambda e: token_copy(e, e).wait_recv())
    each(n_fs - 1, lambda i: send_up(jnp.bitwise_xor(f, offset(i))))
    send_down(0)

    def span(tp):
        return incoming.at[:, pl.ds(0, CAP), pl.ds(aligned(tp * columns), columns)]

    def line(d, chip):
        other = jnp.bitwise_xor(x, d)
        return remote(
            span(chip * 2 + core), span(chip * 2 + core), line_ss.at[d - 1], line_rs.at[d - 1], f, other * 2 + core
        )

    def pair(d, on):
        chip = jnp.bitwise_xor(x, d)
        return remote(
            span(chip * 2 + on), span(chip * 2 + on), pair_ss.at[d], pair_rs.at[d], f, x * 2 + 1 - core
        )

    for d in range(1, chips):
        line(d, x).start()
    pair(0, core).start()
    for d in range(1, chips):
        line(d, jnp.bitwise_xor(x, d)).wait_recv()
        pair(d, core).start()
    for d in range(chips):
        pair(d, 1 - core).wait_recv()

    peers(lambda e: weight_copy(gate_send, gate_recv, gate_ss, gate_rs, e, e).wait_recv())
    peers(lambda e: weight_copy(up_send, up_recv, up_ss, up_rs, e, e).wait_recv())
    each(chunks - 1, lambda c: send_down(c + 1))
    tile = 256
    width = incoming.shape[2]
    group = 2

    def hidden_step(i):
        g, n = i // (units // tile), i % (units // tile)
        lanes = pl.ds(aligned(n * tile, tile), tile)
        at = pl.ds(g * group, group)
        received = incoming[at].reshape(group * ROWS, width)
        gate_pre = jnp.dot(received, gate_recv[:, lanes], preferred_element_type=F32)
        up_pre = jnp.dot(received, up_recv[:, lanes], preferred_element_type=F32)
        value = gate_pre / (1.0 + jnp.exp(-gate_pre)) * up_pre
        hidden[at, :, lanes] = value.astype(BF16).reshape(group, ROWS, tile)

    each(n_fs // group * (units // tile), hidden_step)

    def far_copy(c):
        return remote(far, far_recv.at[c], far_ss.at[c], far_rs.at[c], f, x * 2 + 1 - core)

    def across_copy(c, d):
        other = jnp.bitwise_xor(x, d)
        return remote(
            near.at[c % 2, other], across_recv.at[c, d - 1], across_ss.at[c, d - 1], across_rs.at[c, d - 1],
            f, other * 2 + core,
        )

    def back_copy(c, e, owner):
        return remote(
            back_send.at[c, e, pl.ds(0, CAP)],
            back_recv.at[c, owner, pl.ds(0, CAP)],
            back_ss.at[c, e],
            back_rs.at[c, owner],
            e,
            t,
        )

    def send_back(c):
        peers(lambda e: back_copy(c, e, f).start())

    def product(c, side, store):
        taken = jnp.concatenate([down_recv[:, place(c, 2 * chip + side)] for chip in range(chips)], axis=1)

        def step(g):
            at = pl.ds(g * group, group)
            value = jnp.dot(
                hidden[at].reshape(group * ROWS, units), taken, preferred_element_type=F32
            ).astype(BF16)
            for chip in range(chips):
                store(chip, at, value[:, chip * LANES : (chip + 1) * LANES].reshape(group, ROWS, LANES))

        each(n_fs // group, step)

    def store_far(chip, at, value):
        far[chip, at] = value

    def finish(c):
        for d in range(1, chips):
            across_copy(c, d).wait_recv()

        def one(e):
            value = near[c % 2, x, e].astype(F32) + far_recv[c, x, e].astype(F32)
            for d in range(1, chips):
                value = value + across_recv[c, d - 1, e].astype(F32)
            back_send[c, e] = value.astype(BF16)

        each(n_fs, one)
        back_recv[c, f, pl.ds(0, CAP), :] = back_send[c, f, pl.ds(0, CAP), :]

    def down_chunk(c):
        def store_near(chip, at, value):
            near[c % 2, chip, at] = value

        def arrival(i):
            fs, tp = t * ratio + i // n_tp, i % n_tp

            @pl.when(jnp.logical_not((fs == f) & (tp == t)))
            def _():
                down_copy(c, f, t, fs, tp).wait_recv()

        each(ratio * n_tp, arrival)


        product(c, 1 - core, store_far)
        far_copy(c).start()

        @pl.when(c > 1)
        def _():
            for d in range(1, chips):
                across_copy(c - 2, d).wait_send()

        product(c, core, store_near)
        far_copy(c).wait()
        for d in range(1, chips):
            other = jnp.bitwise_xor(x, d)

            def add(e):
                total = near[c % 2, other, e].astype(F32) + far_recv[c, other, e].astype(F32)
                near[c % 2, other, e] = total.astype(BF16)

            each(n_fs, add)
            across_copy(c, d).start()

        @pl.when(c > 0)
        def _():
            finish(c - 1)
            send_back(c - 1)

    each(chunks, down_chunk)
    finish(chunks - 1)
    send_back(chunks - 1)
    for c in range(chunks - 2, chunks):
        for d in range(1, chips):
            across_copy(c, d).wait_send()

    def combine(c):
        peers(lambda e: back_copy(c, e, e).wait_recv())
        result[:, pl.ds(aligned(c * LANES), LANES)] = weighted(slot, share, lambda e: back_recv[c, e])

    each(chunks - 1, combine)
    peers(lambda e: back_copy(chunks - 1, e, e).wait_recv())

    peers(lambda e: weight_copy(gate_send, gate_recv, gate_ss, gate_rs, e, f).wait_send())
    peers(lambda e: weight_copy(up_send, up_recv, up_ss, up_rs, e, f).wait_send())
    peers(lambda e: token_copy(e, f).wait_send())
    for d in range(1, chips):
        line(d, x).wait_send()
    for d in range(chips):
        pair(d, core).wait_send()

    def drain(c):
        def one(e):
            @pl.when(jnp.logical_not((e == f) & (owner == t)))
            def _():
                down_copy(c, e, owner, f, t).wait_send()

        each(n_fs, one)
        peers(lambda e: back_copy(c, e, f).wait_send())

    each(chunks, drain)


def body(tokens, routes, route_weight, norm_gain, gate_master, up_master, down_master):
    n_fs, n_tp = lax.axis_size("fs"), lax.axis_size("tp")
    count, width = tokens.shape
    experts, rows, units = gate_master.shape
    part, columns = down_master.shape[1:]
    chips, chunks, ratio = n_tp // 2, columns // LANES, n_fs // n_tp
    assert experts == n_fs
    dma = pltpu.SemaphoreType.DMA
    lines = max(1, chips - 1)
    scratch = [
        pltpu.VMEM((n_fs, rows, units), BF16),
        pltpu.VMEM((n_fs, rows, units), BF16),
        pltpu.VMEM((chunks, n_fs, part, LANES), BF16),
        pltpu.VMEM((STAGES, rows, units), F32),
        pltpu.VMEM((2, part, columns), F32),
        pltpu.VMEM((2, count // 8, width), BF16),
        pltpu.VMEM((count, columns), BF16),
        pltpu.VMEM((n_fs, ROWS, columns), BF16),
        pltpu.VMEM((n_fs, ROWS, width), BF16),
        pltpu.VMEM((n_fs, ROWS, units), BF16),
        pltpu.VMEM((chips, n_fs, ROWS, LANES), BF16),
        pltpu.VMEM((chunks, chips, n_fs, ROWS, LANES), BF16),
        pltpu.VMEM((2, chips, n_fs, ROWS, LANES), BF16),
        pltpu.VMEM((chunks, lines, n_fs, ROWS, LANES), BF16),
        pltpu.VMEM((chunks, n_fs, ROWS, LANES), BF16),
        pltpu.VMEM((1, rows), F32),
        pltpu.VMEM((rows, LANES), F32),
        pltpu.VMEM((2, count), jnp.int32),
        pltpu.VMEM((2, count), F32),
        pltpu.VMEM((n_fs, count), F32),
        dma((STAGES,)), dma((2,)), dma((3,)), dma((2,)),
        dma((n_fs,)), dma((n_fs,)), dma((n_fs,)), dma((n_fs,)), dma((n_fs,)), dma((n_fs,)),
        dma((chunks, n_fs)), dma((chunks, ratio * n_tp)),
        dma((lines,)), dma((lines,)), dma((chips,)), dma((chips,)),
        dma((chunks,)), dma((chunks,)), dma((chunks, lines)), dma((chunks, lines)),
        dma((chunks, n_fs)), dma((chunks, n_fs)),
    ]
    shapes = (
        (n_fs * rows, units), (n_fs * rows, units), (ratio * part, n_tp * columns), (count, columns)
    )
    kept = sum(2 * a * b for a, b in shapes) + 2 * chunks * n_fs * DEPTH * LANES + 8 * count * LANES
    anywhere, vector = pl.BlockSpec(memory_space=pl.ANY), pl.BlockSpec(memory_space=pltpu.VMEM)
    held = pl.pallas_call(
        functools.partial(kernel, n_fs, n_tp),
        out_shape=(
            *(pltpu.VMEM(shape, BF16) for shape in shapes),
            pltpu.VMEM((chunks, n_fs, DEPTH, LANES), BF16),
            pltpu.VMEM((count, n_fs), F32),
            pltpu.VMEM((count, n_fs), F32),
        ),
        in_specs=[anywhere] * 7,
        out_specs=(vector,) * 7,
        scratch_shapes=scratch,
        compiler_params=pltpu.CompilerParams(
            collective_id=0, has_side_effects=True, vmem_limit_bytes=VMEM - kept
        ),
        name="layer",
    )(routes.T, route_weight.T, norm_gain[None], tokens, gate_master, up_master, down_master)
    return pl.pallas_call(
        store_kernel,
        out_shape=tuple(jax.ShapeDtypeStruct(shape, BF16) for shape in shapes),
        in_specs=[vector] * 7,
        out_specs=(anywhere,) * 4,
        scratch_shapes=[pltpu.VMEM((count, LANES), BF16), dma((5,))],
        compiler_params=pltpu.CompilerParams(vmem_limit_bytes=16 * 1000 * 1000),
        name="store",
    )(*(pltpu.with_memory_space_constraint(value, pltpu.VMEM) for value in held))


def solution(mesh):
    placed = (
        P("fs", None),
        P("fs", None),
        P("fs", None),
        P("fs"),
        P(None, "fs", "tp"),
        P(None, "fs", "tp"),
        P(None, "fs", "tp"),
    )

    def step(*args):
        gate, up, down, out = body(*args)
        return gate[None], up[None], down[None], out

    return jax.shard_map(
        step,
        mesh=mesh,
        in_specs=placed,
        out_specs=(P("fs", None, "tp"), P("fs", None, "tp"), P("fs", "tp", None), P("fs", "tp")),
        check_vma=False,
    )
```

```python
import functools

import jax
import jax.numpy as jnp
from jax import lax
from jax.experimental import pallas as pl
from jax.experimental.pallas import tpu as pltpu
from jax.sharding import PartitionSpec as P

CAP = 216
ROWS = 224
DEPTH = 256
LANES = 128
STAGES = 3
VMEM = 67 * 1000 * 1000
MESH = pl.DeviceIdType.MESH
F32, BF16 = jnp.float32, jnp.bfloat16


def aligned(value, step=LANES):
    return pl.multiple_of(value, step)


def weighted(slot, share, rows_of):
    count, n_fs = slot.shape
    lane_id = lax.broadcasted_iota(jnp.int32, (count, DEPTH), 1).astype(F32)
    value = jnp.zeros((count, LANES), F32)
    for e in range(n_fs):
        pick = jnp.where(lane_id == slot[:, e : e + 1], 1.0, 0.0).astype(BF16)
        value = value + share[:, e : e + 1] * jnp.dot(pick, rows_of(e), preferred_element_type=F32)
    return value.astype(BF16)


def store_kernel(gate, up, down, result, back, slot, share, gate_out, up_out, down_out, layer_out, last, sem):
    early = result.shape[1] - LANES
    copies = [
        pltpu.make_async_copy(gate, gate_out, sem.at[0]),
        pltpu.make_async_copy(up, up_out, sem.at[1]),
        pltpu.make_async_copy(down, down_out, sem.at[2]),
        pltpu.make_async_copy(result.at[:, pl.ds(0, early)], layer_out.at[:, pl.ds(0, early)], sem.at[3]),
    ]
    for copy in copies:
        copy.start()
    chunk = back.shape[0] - 1
    last[...] = weighted(slot, share, lambda e: back[chunk, e])
    copies.append(pltpu.make_async_copy(last, layer_out.at[:, pl.ds(early, LANES)], sem.at[4]))
    copies[-1].start()
    for copy in copies:
        copy.wait()


def kernel(
    n_fs, n_tp, routes_in, weight_in, gain_in, tokens_in, gate_in, up_in, down_in,
    gate_recv, up_recv, down_recv, result, back_recv, slot, share,
    gate_send, up_send, down_send, stage, down_stage,
    tokens, normed, outgoing, incoming, hidden, far, far_recv, near, across_recv,
    back_send, gain_row, gain, routes, weight, slot_across,
    load_sem, down_load_sem, small_sem, token_load_sem, gate_ss, gate_rs, up_ss, up_rs, token_ss, token_rs,
    down_ss, down_rs, line_ss, line_rs, pair_ss, pair_rs, far_ss, far_rs, across_ss, across_rs,
    back_ss, back_rs,
):
    f, t = lax.axis_index("fs"), lax.axis_index("tp")
    core, x = t % 2, t // 2
    chips = n_tp // 2
    ratio = n_fs // n_tp
    rows, units = gate_send.shape[1:]
    part = down_stage.shape[1]
    columns = down_stage.shape[2]
    chunks = columns // LANES
    half = n_fs // 2

    def remote(src, dst, ss, rs, fs, tp):
        return pltpu.make_async_remote_copy(
            src_ref=src, dst_ref=dst, send_sem=ss, recv_sem=rs,
            device_id={"fs": fs, "tp": tp}, device_id_type=MESH,
        )

    def each(n, action):
        def step(i, carry):
            action(i)
            return carry

        lax.fori_loop(0, n, step, 0)

    def offset(i):
        return jnp.where(i < half, i + half, jnp.where(i == n_fs - 1, 0, i - half + 1))

    small = [
        pltpu.make_async_copy(gain_in, gain_row, small_sem.at[0]),
        pltpu.make_async_copy(routes_in, routes, small_sem.at[1]),
        pltpu.make_async_copy(weight_in, weight, small_sem.at[2]),
    ]
    small[0].start()

    def load(source, i):
        return pltpu.make_async_copy(
            source.at[jnp.bitwise_xor(f, offset(i))], stage.at[i % STAGES], load_sem.at[i % STAGES]
        )

    for i in range(STAGES):
        load(gate_in, i).start()
    for copy in small[1:]:
        copy.start()
    strip = tokens.shape[1]
    count = normed.shape[0]

    def token_load(i):
        return pltpu.make_async_copy(
            tokens_in.at[pl.ds(aligned(i * strip, strip), strip)], tokens.at[i % 2], token_load_sem.at[i % 2]
        )

    token_load(0).start()
    token_load(1).start()

    barrier = pltpu.get_barrier_semaphore()
    total = n_fs * n_tp
    me = f * n_tp + t

    def greet(i):
        other = (me + i + 1) % total
        pl.semaphore_signal(
            barrier, inc=1, device_id={"fs": other // n_tp, "tp": other % n_tp}, device_id_type=MESH
        )

    each(total - 1, greet)

    back_recv[:, :, CAP:, :] = jnp.zeros((chunks, n_fs, DEPTH - CAP, LANES), BF16)

    small[0].wait()
    same = lax.broadcasted_iota(jnp.int32, (rows, rows), 0) == lax.broadcasted_iota(jnp.int32, (rows, rows), 1)
    column = jnp.sum(jnp.where(same, gain_row[...], 0.0), axis=1, keepdims=True)
    gain[...] = jnp.broadcast_to(column, (rows, LANES))

    def weight_copy(send, recv, ss, rs, e, owner):
        return remote(
            send.at[e], recv.at[pl.ds(aligned(owner * rows), rows)], ss.at[e], rs.at[owner], e, t
        )

    def scaled(block):
        scale = gain[...]
        return jnp.concatenate(
            [(block[:, k : k + LANES] * scale).astype(BF16) for k in range(0, units, LANES)], axis=1
        )

    def cast_weights(source, send, recv, sent):
        def step(i):
            e = jnp.bitwise_xor(f, offset(i))
            load(source, i).wait()
            cast = scaled(stage[i % STAGES])

            @pl.when(i < n_fs - 1)
            def _():
                send[e] = cast

            @pl.when(i == n_fs - 1)
            def _():
                recv[pl.ds(aligned(f * rows), rows), :] = cast

            @pl.when(i + STAGES < n_fs)
            def _():
                load(source, i + STAGES).start()

        def send_step(i):
            step(i)
            sent(jnp.bitwise_xor(f, offset(i - 1)))

        if sent is None:
            each(n_fs, step)
        else:
            each(2, step)
            pl.semaphore_wait(barrier, total - 1)
            sent(jnp.bitwise_xor(f, offset(0)))
            each(n_fs - 2, lambda i: send_step(i + 2))

    def send_gate(e):
        weight_copy(gate_send, gate_recv, gate_ss, gate_rs, e, f).start()

    def send_up(e):
        weight_copy(up_send, up_recv, up_ss, up_rs, e, f).start()

    cast_weights(gate_in, gate_send, gate_recv, send_gate)
    for i in range(STAGES):
        load(up_in, i).start()

    for copy in small[1:3]:
        copy.wait()
    row_id = lax.broadcasted_iota(jnp.int32, (count, count), 0)
    column_id = lax.broadcasted_iota(jnp.int32, (count, count), 1)
    expert_row = lax.broadcasted_iota(jnp.int32, (n_fs, count), 0)
    first, second = expert_row == routes[0:1, :], expert_row == routes[1:2, :]
    named = first | second
    before = jnp.dot(
        jnp.where(named, 1.0, 0.0).astype(BF16),
        jnp.where(row_id < column_id, 1.0, 0.0).astype(BF16),
        preferred_element_type=F32,
    )
    before = jnp.where(named, before, -1.0)
    slot_across[...] = before
    slot[...] = before.T
    share[...] = (jnp.where(first, weight[0:1, :], 0.0) + jnp.where(second, weight[1:2, :], 0.0)).T

    def norm(i):
        at = pl.ds(aligned(i * strip, strip), strip)
        token_load(i).wait()
        values = tokens[i % 2].astype(F32)
        scale = lax.rsqrt(jnp.mean(values * values, axis=1, keepdims=True) + 1e-06)
        mine = tokens[i % 2, :, pl.ds(aligned(t * columns), columns)].astype(F32)
        normed[at, :] = (mine * scale).astype(BF16)

        @pl.when(i + 2 < count // strip)
        def _():
            token_load(i + 2).start()

    each(count // strip, norm)

    def token_copy(e, owner):
        return remote(
            outgoing.at[e, pl.ds(0, CAP)],
            incoming.at[owner, pl.ds(0, CAP), pl.ds(aligned(t * columns), columns)],
            token_ss.at[e],
            token_rs.at[owner],
            e,
            t,
        )

    slot_id = lax.broadcasted_iota(jnp.int32, (ROWS, count), 0).astype(F32)

    def dispatch(i):
        e = jnp.bitwise_xor(f, offset(i))
        pick = jnp.where(slot_id == slot_across[pl.ds(e, 1), :], 1.0, 0.0).astype(BF16)
        picked = jnp.dot(pick, normed[...], preferred_element_type=F32).astype(BF16)

        @pl.when(i < n_fs - 1)
        def _():
            outgoing[e] = picked

        @pl.when(i == n_fs - 1)
        def _():
            incoming[f, :, pl.ds(aligned(t * columns), columns)] = picked

        @pl.when(i > 0)
        def _():
            token_copy(jnp.bitwise_xor(f, offset(i - 1)), f).start()

    each(n_fs, dispatch)

    cast_weights(up_in, up_send, up_recv, None)

    def down_load(i):
        return pltpu.make_async_copy(down_in.at[i], down_stage.at[i % 2], down_load_sem.at[i % 2])

    owner = f // ratio

    def place(c, tp):
        return pl.ds(aligned(tp * columns + c * LANES), LANES)

    def down_copy(c, e, to, fs, tp):
        return remote(
            down_send.at[c, e],
            down_recv.at[pl.ds(aligned(fs % ratio * part), part), place(c, tp)],
            down_ss.at[c, e],
            down_rs.at[c, fs % ratio * n_tp + tp],
            e,
            to,
        )

    down_load(0).start()
    down_load(1).start()

    def down_cast(i):
        down_load(i).wait()
        for c in range(chunks):
            down_send[c, i] = down_stage[i % 2, :, c * LANES : (c + 1) * LANES].astype(BF16)

        @pl.when(i + 2 < n_fs)
        def _():
            down_load(i + 2).start()

    each(n_fs, down_cast)

    def send_down(c):
        def one(i):
            e = jnp.bitwise_xor(f, offset(i))
            mine = (e == f) & (owner == t)

            @pl.when(mine)
            def _():
                down_recv[pl.ds(aligned(f % ratio * part), part), place(c, t)] = down_send[c, e]

            @pl.when(jnp.logical_not(mine))
            def _():
                down_copy(c, e, owner, f, t).start()

        each(n_fs, one)

    def peers(action):
        each(n_fs - 1, lambda i: action(jnp.bitwise_xor(f, i + 1)))

    peers(lambda e: token_copy(e, e).wait_recv())
    each(n_fs - 1, lambda i: send_up(jnp.bitwise_xor(f, offset(i))))
    send_down(0)

    def span(tp):
        return incoming.at[:, pl.ds(0, CAP), pl.ds(aligned(tp * columns), columns)]

    def line(d, chip):
        other = jnp.bitwise_xor(x, d)
        return remote(
            span(chip * 2 + core), span(chip * 2 + core), line_ss.at[d - 1], line_rs.at[d - 1], f, other * 2 + core
        )

    def pair(d, on):
        chip = jnp.bitwise_xor(x, d)
        return remote(
            span(chip * 2 + on), span(chip * 2 + on), pair_ss.at[d], pair_rs.at[d], f, x * 2 + 1 - core
        )

    for d in range(1, chips):
        line(d, x).start()
    pair(0, core).start()
    for d in range(1, chips):
        line(d, jnp.bitwise_xor(x, d)).wait_recv()
        pair(d, core).start()
    for d in range(chips):
        pair(d, 1 - core).wait_recv()

    peers(lambda e: weight_copy(gate_send, gate_recv, gate_ss, gate_rs, e, e).wait_recv())
    peers(lambda e: weight_copy(up_send, up_recv, up_ss, up_rs, e, e).wait_recv())
    each(chunks - 1, lambda c: send_down(c + 1))
    tile = 256
    width = incoming.shape[2]
    group = 2

    def hidden_step(i):
        g, n = i // (units // tile), i % (units // tile)
        lanes = pl.ds(aligned(n * tile, tile), tile)
        at = pl.ds(g * group, group)
        received = incoming[at].reshape(group * ROWS, width)
        gate_pre = jnp.dot(received, gate_recv[:, lanes], preferred_element_type=F32)
        up_pre = jnp.dot(received, up_recv[:, lanes], preferred_element_type=F32)
        value = gate_pre / (1.0 + jnp.exp(-gate_pre)) * up_pre
        hidden[at, :, lanes] = value.astype(BF16).reshape(group, ROWS, tile)

    each(n_fs // group * (units // tile), hidden_step)

    def first(part_id):
        return jnp.bitwise_xor(f // half, 1 - part_id) * half

    def senders(part_id):
        return pl.ds(first(part_id), half)

    def far_copy(c, part_id):
        return remote(
            far.at[:, senders(part_id)], far_recv.at[c, :, senders(part_id)],
            far_ss.at[c, part_id], far_rs.at[c, part_id], f, x * 2 + 1 - core,
        )

    def across_copy(c, d, part_id):
        other = jnp.bitwise_xor(x, d)
        return remote(
            near.at[c % 2, other, senders(part_id)], across_recv.at[c, d - 1, senders(part_id)],
            across_ss.at[c, 2 * (d - 1) + part_id], across_rs.at[c, 2 * (d - 1) + part_id],
            f, other * 2 + core,
        )

    def back_copy(c, e, owner):
        return remote(
            back_send.at[c, e, pl.ds(0, CAP)],
            back_recv.at[c, owner, pl.ds(0, CAP)],
            back_ss.at[c, e],
            back_rs.at[c, owner],
            e,
            t,
        )

    def send_back(c, part_id):
        if part_id == 0:
            each(half, lambda i: back_copy(c, jnp.bitwise_xor(f, half + i), f).start())
        else:
            each(half - 1, lambda i: back_copy(c, jnp.bitwise_xor(f, i + 1), f).start())

    def product(c, side, part_id, store):
        taken = jnp.concatenate([down_recv[:, place(c, 2 * chip + side)] for chip in range(chips)], axis=1)

        def step(g):
            at = pl.ds(first(part_id) + g * group, group)
            value = jnp.dot(
                hidden[at].reshape(group * ROWS, units), taken, preferred_element_type=F32
            ).astype(BF16)
            for chip in range(chips):
                store(chip, at, value[:, chip * LANES : (chip + 1) * LANES].reshape(group, ROWS, LANES))

        each(half // group, step)

    def store_far(chip, at, value):
        far[chip, at] = value

    def finish(c):
        for part_id in range(2):
            for d in range(1, chips):
                across_copy(c, d, part_id).wait_recv()

            def one(i):
                e = first(part_id) + i
                value = near[c % 2, x, e].astype(F32) + far_recv[c, x, e].astype(F32)
                for d in range(1, chips):
                    value = value + across_recv[c, d - 1, e].astype(F32)
                back_send[c, e] = value.astype(BF16)

            each(half, one)
            send_back(c, part_id)
        back_recv[c, f, pl.ds(0, CAP), :] = back_send[c, f, pl.ds(0, CAP), :]

    def down_chunk(c):
        def store_near(chip, at, value):
            near[c % 2, chip, at] = value

        def arrival(i):
            fs, tp = t * ratio + i // n_tp, i % n_tp

            @pl.when(jnp.logical_not((fs == f) & (tp == t)))
            def _():
                down_copy(c, f, t, fs, tp).wait_recv()

        each(ratio * n_tp, arrival)


        @pl.when(c > 1)
        def _():
            wait_across(c - 2)

        for part_id in range(2):
            product(c, 1 - core, part_id, store_far)
            far_copy(c, part_id).start()
            product(c, core, part_id, store_near)
            far_copy(c, part_id).wait()
            for d in range(1, chips):
                other = jnp.bitwise_xor(x, d)

                def add(i):
                    e = first(part_id) + i
                    value = near[c % 2, other, e].astype(F32) + far_recv[c, other, e].astype(F32)
                    near[c % 2, other, e] = value.astype(BF16)

                each(half, add)
                across_copy(c, d, part_id).start()

        @pl.when(c > 0)
        def _():
            finish(c - 1)

    def wait_across(c):
        for part_id in range(2):
            for d in range(1, chips):
                across_copy(c, d, part_id).wait_send()

    each(chunks, down_chunk)
    finish(chunks - 1)
    for c in range(chunks - 2, chunks):
        wait_across(c)

    def combine(c):
        peers(lambda e: back_copy(c, e, e).wait_recv())
        result[:, pl.ds(aligned(c * LANES), LANES)] = weighted(slot, share, lambda e: back_recv[c, e])

    each(chunks - 1, combine)

    peers(lambda e: weight_copy(gate_send, gate_recv, gate_ss, gate_rs, e, f).wait_send())
    peers(lambda e: weight_copy(up_send, up_recv, up_ss, up_rs, e, f).wait_send())
    peers(lambda e: token_copy(e, f).wait_send())
    for d in range(1, chips):
        line(d, x).wait_send()
    for d in range(chips):
        pair(d, core).wait_send()

    def drain(c):
        def one(e):
            @pl.when(jnp.logical_not((e == f) & (owner == t)))
            def _():
                down_copy(c, e, owner, f, t).wait_send()

        each(n_fs, one)

    each(chunks, drain)
    each(chunks, lambda c: peers(lambda e: back_copy(c, e, f).wait_send()))
    peers(lambda e: back_copy(chunks - 1, e, e).wait_recv())


def body(tokens, routes, route_weight, norm_gain, gate_master, up_master, down_master):
    n_fs, n_tp = lax.axis_size("fs"), lax.axis_size("tp")
    count, width = tokens.shape
    experts, rows, units = gate_master.shape
    part, columns = down_master.shape[1:]
    chips, chunks, ratio = n_tp // 2, columns // LANES, n_fs // n_tp
    assert experts == n_fs
    dma = pltpu.SemaphoreType.DMA
    lines = max(1, chips - 1)
    scratch = [
        pltpu.VMEM((n_fs, rows, units), BF16),
        pltpu.VMEM((n_fs, rows, units), BF16),
        pltpu.VMEM((chunks, n_fs, part, LANES), BF16),
        pltpu.VMEM((STAGES, rows, units), F32),
        pltpu.VMEM((2, part, columns), F32),
        pltpu.VMEM((2, count // 8, width), BF16),
        pltpu.VMEM((count, columns), BF16),
        pltpu.VMEM((n_fs, ROWS, columns), BF16),
        pltpu.VMEM((n_fs, ROWS, width), BF16),
        pltpu.VMEM((n_fs, ROWS, units), BF16),
        pltpu.VMEM((chips, n_fs, ROWS, LANES), BF16),
        pltpu.VMEM((chunks, chips, n_fs, ROWS, LANES), BF16),
        pltpu.VMEM((2, chips, n_fs, ROWS, LANES), BF16),
        pltpu.VMEM((chunks, lines, n_fs, ROWS, LANES), BF16),
        pltpu.VMEM((chunks, n_fs, ROWS, LANES), BF16),
        pltpu.VMEM((1, rows), F32),
        pltpu.VMEM((rows, LANES), F32),
        pltpu.VMEM((2, count), jnp.int32),
        pltpu.VMEM((2, count), F32),
        pltpu.VMEM((n_fs, count), F32),
        dma((STAGES,)), dma((2,)), dma((3,)), dma((2,)),
        dma((n_fs,)), dma((n_fs,)), dma((n_fs,)), dma((n_fs,)), dma((n_fs,)), dma((n_fs,)),
        dma((chunks, n_fs)), dma((chunks, ratio * n_tp)),
        dma((lines,)), dma((lines,)), dma((chips,)), dma((chips,)),
        dma((chunks, 2)), dma((chunks, 2)), dma((chunks, 2 * lines)), dma((chunks, 2 * lines)),
        dma((chunks, n_fs)), dma((chunks, n_fs)),
    ]
    shapes = (
        (n_fs * rows, units), (n_fs * rows, units), (ratio * part, n_tp * columns), (count, columns)
    )
    kept = sum(2 * a * b for a, b in shapes) + 2 * chunks * n_fs * DEPTH * LANES + 8 * count * LANES
    anywhere, vector = pl.BlockSpec(memory_space=pl.ANY), pl.BlockSpec(memory_space=pltpu.VMEM)
    held = pl.pallas_call(
        functools.partial(kernel, n_fs, n_tp),
        out_shape=(
            *(pltpu.VMEM(shape, BF16) for shape in shapes),
            pltpu.VMEM((chunks, n_fs, DEPTH, LANES), BF16),
            pltpu.VMEM((count, n_fs), F32),
            pltpu.VMEM((count, n_fs), F32),
        ),
        in_specs=[anywhere] * 7,
        out_specs=(vector,) * 7,
        scratch_shapes=scratch,
        compiler_params=pltpu.CompilerParams(
            collective_id=0, has_side_effects=True, vmem_limit_bytes=VMEM - kept
        ),
        name="layer",
    )(routes.T, route_weight.T, norm_gain[None], tokens, gate_master, up_master, down_master)
    return pl.pallas_call(
        store_kernel,
        out_shape=tuple(jax.ShapeDtypeStruct(shape, BF16) for shape in shapes),
        in_specs=[vector] * 7,
        out_specs=(anywhere,) * 4,
        scratch_shapes=[pltpu.VMEM((count, LANES), BF16), dma((5,))],
        compiler_params=pltpu.CompilerParams(vmem_limit_bytes=16 * 1000 * 1000),
        name="store",
    )(*(pltpu.with_memory_space_constraint(value, pltpu.VMEM) for value in held))


def solution(mesh):
    placed = (
        P("fs", None),
        P("fs", None),
        P("fs", None),
        P("fs"),
        P(None, "fs", "tp"),
        P(None, "fs", "tp"),
        P(None, "fs", "tp"),
    )

    def step(*args):
        gate, up, down, out = body(*args)
        return gate[None], up[None], down[None], out

    return jax.shard_map(
        step,
        mesh=mesh,
        in_specs=placed,
        out_specs=(P("fs", None, "tp"), P("fs", None, "tp"), P("fs", "tp", None), P("fs", "tp")),
        check_vma=False,
    )
```
